256 devices in a mesh: fs: 16 (over y, x), tp: 16 (over z, core).
Axes of the slice: x: 4, y: 4, z: 8, core: 2. Of those that a mesh axis runs over, the one named last changes fastest.
Arguments:
- tokens: bfloat16 [32768, 2048], P(('fs', 'tp')), may hold values from -6 to 6
- up_weight: bfloat16 [2048, 4096], P('fs', 'tp'), may hold values from -0.125 to 0.125
- down_weight: bfloat16 [4096, 2048], P('tp', 'fs'), may hold values from -0.09375 to 0.09375
- cotangent: bfloat16 [32768, 2048], P(('fs', 'tp')), may hold values from -24 to 24
Outputs:
- input_grad: bfloat16 [32768, 2048], P(('fs', 'tp'))
- up_grad: float32 [2048, 4096], P('fs', 'tp')
- down_grad: float32 [4096, 2048], P('tp', 'fs')
The draws below stay inside these ranges and needn't reach their ends.
All inputs are finite; a program needn't handle non-finite values.
Results may differ from the reference program's by a relative error of at most 0.018.
Values may be sent and summed in bfloat16 or wider, within the bound.
A program may use at most 128 MiB of HBM per device.

```python
import jax
import jax.numpy as jnp
from jax import lax

D = 2048
FF = 4096
TOKENS = 32768
N_TP = 16


def spiked(entries, own_key, source, target, blocks, factor):
    owner, partner = [(jnp.arange(entries.shape[dim]) // (entries.shape[dim] // blocks)).reshape([-1 if axis == dim else 1 for axis in range(entries.ndim)]) for dim in (source, target)]
    chosen = jax.random.permutation(own_key, blocks)[partner]
    strong = (owner == chosen) | (owner == (partner + blocks // 2) % blocks)
    return jnp.where(strong, factor * entries, entries)


def levels(own_key, dims, pieces, low, high):
    loudness = 1.0
    for axis_at, parts in pieces:
        heights = jax.random.uniform(jax.random.fold_in(jax.random.fold_in(own_key, 6), axis_at), (parts,), jnp.float32, low / len(pieces), high / len(pieces))
        loudness = loudness * jnp.repeat(jnp.exp(heights), dims[axis_at] // parts).reshape((-1,) + (1,) * (len(dims) - 1 - axis_at))
    return loudness


def bell_draw(key, shape, spread, reach, split=(), kind=jnp.bfloat16):
    level = levels(key, shape, split, -0.22, 0.18) if split else 1.0
    drawn = jax.random.normal(key, shape, jnp.float32) * spread * level
    return jnp.minimum(jnp.maximum(drawn, -reach), reach).astype(kind)


def gaussian_with(rng, dims, spread, bound, pieces, heavy, held_as=jnp.bfloat16):
    values = spread * jax.random.normal(rng, dims, jnp.float32)
    if pieces:
        values = values * levels(rng, dims, pieces, -0.22, 0.18)
    return jnp.clip(spiked(values, jax.random.fold_in(rng, 3), *heavy), -bound, bound).astype(held_as)


def setup_inputs(seed: int = 0) -> dict:
    key_list = jax.random.split(jax.random.key(seed), 5)
    return {
        "tokens": bell_draw(key_list[0], (TOKENS, D), 1.0, 6.0, ((0, 256),)),
        "up_weight": bell_draw(key_list[1], (D, FF), D ** -0.5, 0.125, ((0, 16), (1, 16))),
        "down_weight": bell_draw(key_list[2], (FF, D), FF ** -0.5, 0.09375, ((0, 16), (1, 16))),
        "cotangent": gaussian_with(key_list[3], (TOKENS, D), 1.0, 24.0, ((0, 256),), (0, 1, 256, 6.0)),
    }


def reference(tokens, up_weight, down_weight, cotangent):
    pre = jnp.dot(tokens, up_weight, preferred_element_type=jnp.float32)
    active = jnp.maximum(pre, 0.0)
    hidden = (active * active).astype(jnp.bfloat16)
    dhidden = jnp.dot(cotangent, down_weight.T, preferred_element_type=jnp.float32)
    dpre = (2.0 * active * dhidden).astype(jnp.bfloat16)
    factor = 1.0 / jnp.sqrt(jnp.float32(TOKENS))
    down_grad = jnp.dot(hidden.T, cotangent, preferred_element_type=jnp.float32) * factor
    up_grad = jnp.dot(tokens.T, dpre, preferred_element_type=jnp.float32) * factor
    width = FF // N_TP

    def add_block(index, total):
        start = (index * width).astype(jnp.int32)
        cols = lax.dynamic_slice_in_dim(dpre, start, width, 1)
        right = lax.dynamic_slice_in_dim(up_weight, start, width, 1)
        part = jnp.dot(cols, right.T, preferred_element_type=jnp.float32).astype(jnp.bfloat16)
        part = lax.optimization_barrier(part)
        return total + part.astype(jnp.float32)
    total = lax.fori_loop(jnp.int32(0), jnp.int32(N_TP), add_block, jnp.zeros((TOKENS, D), jnp.float32))
    return (total.astype(jnp.bfloat16), up_grad, down_grad)
```

```python
import jax
import jax.numpy as jnp
from jax import lax
from jax.experimental import pallas as pl
from jax.experimental.pallas import tpu as pltpu
from jax.sharding import PartitionSpec as P

BF = jnp.bfloat16
F32 = jnp.float32
MESH = pl.DeviceIdType.MESH

SX, ZP, ZM, YP, YM, YF = 0, 8, 16, 24, 40, 56
TP, TM, TF, TC = 60, 62, 64, 66
GY, GC, GA, GB, FS = 74, 82, 98, 106, 114
XC, XY = 116, 118
FSS = 124
N_SEM = 132


def both(n, body):
    def step(i, carry):
        body(i)
        return carry

    lax.fori_loop(0, n, step, 0)


def kernel(
    factor, tok_in, up_in, dn_in, cot_in, ig_out, ug_out, dg_out,
    X, WS, W, DP, TT, G, RY, RC, ZA, ZB, FX, S, RP, XR, ssem, rsem, lsem,
):
    fs, tp = lax.axis_index("fs"), lax.axis_index("tp")
    y, x = fs // 4, fs % 4
    z, c = tp // 2, tp % 2
    p = lax.rem(z - x + 8, 4)
    xp, xm, xo = (x + 1) % 4, (x + 3) % 4, (x + 2) % 4
    yp, ym, yo = (y + 1) % 4, (y + 3) % 4, (y + 2) % 4
    zp, zm = (z + 1) % 8, (z + 7) % 8

    def dev(yy, xx, zz, cc):
        return (yy * 4 + xx, zz * 2 + cc)

    XP, XM, XO = dev(y, xp, z, c), dev(y, xm, z, c), dev(y, xo, z, c)
    YPd, YMd = dev(yp, x, z, c), dev(ym, x, z, c)
    ZPd, ZMd = dev(y, x, zp, c), dev(y, x, zm, c)
    PA = dev(y, x, z, 1 - c)

    def copy(src, dst, to, sid, sent_id=None):
        sent_id = sid if sent_id is None else sent_id
        return pltpu.make_async_remote_copy(
            src_ref=src, dst_ref=dst, send_sem=ssem.at[sent_id], recv_sem=rsem.at[sid],
            device_id=to, device_id_type=MESH,
        )

    def got(ref, sid):
        copy(ref, ref, PA, sid).wait_recv()

    def sent(ref, sid):
        copy(ref, ref, PA, sid).wait_send()

    crow = pl.ds(pl.multiple_of(c * 128, 128), 128)
    own = [pltpu.make_async_copy(a, X.at[w, x, crow, :], lsem.at[w]) for w, a in enumerate((tok_in, cot_in))]
    for o in own:
        o.start()
    WS[0] = up_in[...]
    WS[1] = dn_in[...].astype(F32).T.astype(BF)

    barrier = pltpu.get_barrier_semaphore()
    for to in (XP, XM, XO, YPd, YMd, ZPd, ZMd, PA):
        pl.semaphore_signal(barrier, inc=1, device_id=to, device_id_type=MESH)
    pl.semaphore_wait(barrier, 8)

    def wrow(yy, j):
        return pl.ds(pl.multiple_of(yy * 512 + j * 128, 128), 128)

    def wpiece(slot, w, yy, j):
        return W.at[slot, w, wrow(yy, j), :]

    @pl.when(p != 0)
    def _():
        for w in range(2):
            copy(WS.at[w], wpiece(0, w, y, x), dev(y, (x + p) % 4, z, c), SX + w * 4 + x).start()

    for o in own:
        o.wait()

    def xblock(w, xx, cc_row):
        return X.at[w, xx, cc_row, :]

    for w, to, base in ((0, XP, TP), (1, XM, TM), (1, XP, TP), (0, XM, TM)):
        copy(xblock(w, x, crow), xblock(w, x, crow), to, base + w).start()
    for w in range(2):
        copy(xblock(w, x, crow), xblock(w, x, crow), PA, TC + w * 4).start()

    @pl.when(p == 0)
    def _():
        for w in range(2):
            W[0, w, wrow(y, x), :] = WS[w]

    def ysend(slot, k, w, j):
        piece = wpiece(slot, w, y, j)
        copy(piece, piece, YPd, YP + slot * 8 + k).start()
        copy(piece, piece, YMd, YM + slot * 8 + k).start()

    def step_a(k):
        w, j = k // 4, k % 4

        @pl.when((p == 0) & (j != x))
        def _():
            got(wpiece(0, w, y, j), SX + k)

        @pl.when(p != 0)
        def _():
            got(wpiece(0, w, y, j), ZP + k)

        copy(wpiece(0, w, y, j), wpiece(jnp.where(p == 3, 1, 0), w, y, j), ZPd, ZP + k).start()

        @pl.when(p == 0)
        def _():
            copy(wpiece(0, w, y, j), wpiece(1, w, y, j), ZMd, ZM + k).start()

        ysend(0, k, w, j)

    def step_b(k):
        w, j = k // 4, k % 4

        @pl.when(p == 0)
        def _():
            got(wpiece(1, w, y, j), ZP + k)

        @pl.when(p != 0)
        def _():
            got(wpiece(1, w, y, j), ZM + k)

        @pl.when(p >= 2)
        def _():
            copy(wpiece(1, w, y, j), wpiece(1, w, y, j), ZMd, ZM + k).start()

        ysend(1, k, w, j)

    lag_a = jnp.where(p == 3, 5, 0)
    lag_b = jnp.where(p == 0, 8, jnp.where(p == 1, 5, 0))

    def zstep(t):
        @pl.when((t >= lag_a) & (t < lag_a + 8))
        def _():
            step_a(t - lag_a)

        @pl.when((t >= lag_b) & (t < lag_b + 8))
        def _():
            step_b(t - lag_b)

    both(8, zstep)
    got(xblock(0, xm, crow), TP)
    copy(xblock(0, xm, crow), xblock(0, xm, crow), XP, TF).start()
    got(xblock(1, xp, crow), TM + 1)
    copy(xblock(1, xp, crow), xblock(1, xp, crow), XM, TF + 1).start()
    both(8, lambda t: zstep(t + 8))

    def wblock(slot, w, yy):
        return W.at[slot, w, pl.ds(pl.multiple_of(yy * 512, 512), 512), :]

    near = jnp.where(p == 3, 1, 0)

    def yforward(i):
        slot = jnp.where(i == 0, near, 1 - near)

        def up(k):
            got(wpiece(slot, 0, ym, k), YP + slot * 8 + k)

        both(4, up)
        copy(wblock(slot, 0, ym), wblock(slot, 0, ym), YPd, YF + slot * 2).start()

        def dn(k):
            got(wpiece(slot, 1, yp, k), YM + slot * 8 + 4 + k)

        both(4, dn)
        copy(wblock(slot, 1, yp), wblock(slot, 1, yp), YMd, YF + slot * 2 + 1).start()

    both(2, yforward)

    def pass_on(w, r):
        xx = (x + r) % 4
        copy(xblock(w, xx, crow), xblock(w, xx, crow), PA, TC + w * 4 + r).start()

    pass_on(0, 3)
    pass_on(1, 1)
    got(xblock(1, xm, crow), TP + 1)
    pass_on(1, 3)
    got(xblock(0, xp, crow), TM)
    pass_on(0, 1)
    got(xblock(0, xo, crow), TF)
    pass_on(0, 2)
    got(xblock(1, xo, crow), TF + 1)
    pass_on(1, 2)

    def yfinish(slot):
        def up(k):
            got(wpiece(slot, 0, yp, k), YM + slot * 8 + k)
            got(wpiece(slot, 1, ym, k), YP + slot * 8 + 4 + k)

        both(4, up)
        for w in range(2):
            got(wblock(slot, w, yo), YF + slot * 2 + w)

    both(2, yfinish)
    orow = pl.ds(pl.multiple_of((1 - c) * 128, 128), 128)
    for w in range(2):
        both(4, lambda r, w=w: got(xblock(w, (x + r) % 4, orow), TC + w * 4 + r))

    def act(i):
        slot, xx = i // 4, i % 4
        pre = jnp.dot(X[0, xx], W[slot, 0], preferred_element_type=F32)
        dh = jnp.dot(X[1, xx], W[slot, 1], preferred_element_type=F32)
        active = jnp.maximum(pre, 0.0)
        hidden = active * active
        dpre = 2.0 * active * dh
        DP[slot, pl.ds(pl.multiple_of(xx * 256, 256), 256), :] = dpre.astype(BF)
        cols = pl.ds(pl.multiple_of(xx * 256, 256), 256)
        TT[slot, 0, :, cols] = dpre.T.astype(BF)
        TT[slot, 1, :, cols] = hidden.T.astype(BF)

    both(8, act)

    first = jnp.where(p < 2, 1, 0)

    def grads(slot):
        def block(i):
            yy = (y + 2 + i) % 4
            cols = pl.ds(pl.multiple_of(yy * 512, 512), 512)
            for w in range(2):
                rows = X[w, :, :, cols].reshape(1024, 512)
                part = jnp.dot(TT[slot, w], rows, preferred_element_type=F32).astype(BF)
                for j in range(4):
                    G[slot, w, yy, j] = part[:, j * 128 : (j + 1) * 128]

        both(4, block)

    def ab(slot):
        base = GY + slot * 4
        copy(G.at[slot, 0, yo], RY.at[slot, 0, 0], YPd, base).start()
        copy(G.at[slot, 1, yo], RY.at[slot, 1, 0], YMd, base + 1).start()
        copy(G.at[slot, 1, yp], RY.at[slot, 0, 1], YPd, base + 2).start()
        copy(G.at[slot, 0, ym], RY.at[slot, 1, 1], YMd, base + 3).start()

    def cstep(slot):
        base = GY + slot * 4
        got(RY.at[slot, 0, 0], base)
        got(RY.at[slot, 1, 0], base + 1)

        def piece(j):
            G[slot, 0, yp, j] = (G[slot, 0, yp, j].astype(F32) + RY[slot, 0, 0, j].astype(F32)).astype(BF)
            copy(G.at[slot, 0, yp, j], RC.at[slot, 0, j], YPd, GC + slot * 8 + j).start()
            G[slot, 1, ym, j] = (G[slot, 1, ym, j].astype(F32) + RY[slot, 1, 0, j].astype(F32)).astype(BF)
            copy(G.at[slot, 1, ym, j], RC.at[slot, 1, j], YMd, GC + slot * 8 + 4 + j).start()

        both(4, piece)

    def yfinal(slot):
        base = GY + slot * 4
        got(RY.at[slot, 0, 1], base + 2)
        got(RY.at[slot, 1, 1], base + 3)

        def piece(j):
            got(RC.at[slot, 0, j], GC + slot * 8 + j)
            G[slot, 0, y, j] = (
                G[slot, 0, y, j].astype(F32) + RC[slot, 0, j].astype(F32) + RY[slot, 1, 1, j].astype(F32)
            ).astype(BF)
            got(RC.at[slot, 1, j], GC + slot * 8 + 4 + j)
            G[slot, 1, y, j] = (
                G[slot, 1, y, j].astype(F32) + RC[slot, 1, j].astype(F32) + RY[slot, 0, 1, j].astype(F32)
            ).astype(BF)

        both(4, piece)

    grads(first)
    ab(first)
    grads(1 - first)

    def igrad(n):
        rows = pl.ds(pl.multiple_of(n * 256, 256), 256)
        nt = (((1,), (1,)), ((), ()))
        part = lax.dot_general(DP[0], W[0, 0, rows, :], nt, preferred_element_type=F32)
        part = part + lax.dot_general(DP[1], W[1, 0, rows, :], nt, preferred_element_type=F32)
        part = part.astype(BF).reshape(4, 2, 128, 256)
        cols = pl.ds(pl.multiple_of((n % 4) * 256, 256), 256)
        for cc in range(2):
            S[cc, n // 4, :, :, cols] = part[:, cc]

    for half in range(2):
        both(4, lambda n, half=half: igrad(half * 4 + n))
        copy(S.at[1 - c, half], RP.at[half], PA, XC + half).start()

    cstep(first)
    ab(1 - first)

    for half in range(2):
        got(RP.at[half], XC + half)

        def add(r, half=half):
            S[c, half, r] = (S[c, half, r].astype(F32) + RP[half, r].astype(F32)).astype(BF)

        both(4, add)
    copy(S.at[c, 0, xo], XR.at[0, 0], XP, XY).start()
    copy(S.at[c, 1, xo], XR.at[1, 0], XM, XY + 1).start()
    copy(S.at[c, 1, xp], XR.at[0, 1], XP, XY + 2).start()
    copy(S.at[c, 0, xm], XR.at[1, 1], XM, XY + 3).start()

    def gpiece(slot, k):
        return G.at[slot, k // 4, y, k % 4]

    def chain_b(k):
        w, j = k // 4, k % 4

        @pl.when(p == 0)
        def _():
            copy(gpiece(1, k), ZA.at[k], ZMd, GA + k).start()

        @pl.when(p >= 2)
        def _():
            got(ZB.at[k], GB + k)
            G[1, w, y, j] = (G[1, w, y, j].astype(F32) + ZB[k].astype(F32)).astype(BF)

        @pl.when(p != 0)
        def _():
            copy(gpiece(1, k), ZB.at[k], ZPd, GB + k).start()

    def chain_a(k):
        w, j = k // 4, k % 4
        got(ZA.at[k], GA + k)

        @pl.when(p != 0)
        def _():
            G[0, w, y, j] = (G[0, w, y, j].astype(F32) + ZA[k].astype(F32)).astype(BF)
            copy(gpiece(0, k), ZA.at[k], ZMd, GA + k).start()

        @pl.when(p == 0)
        def _():
            got(ZB.at[k], GB + k)
            G[0, w, y, j] = (G[0, w, y, j].astype(F32) + ZA[k].astype(F32) + ZB[k].astype(F32)).astype(BF)

            @pl.when(j != x)
            def _():
                copy(gpiece(0, k), FX.at[w], dev(y, j, z, c), FS + w, FSS + k).start()

    def order(k):
        return (k % 2) * 4 + k // 2

    yfinal(first)

    @pl.when(p < 2)
    def _():
        both(8, lambda k: chain_b(order(k)))

    cstep(1 - first)

    @pl.when(p >= 2)
    def _():
        both(8, lambda k: chain_a(order(k)))

    got(XR.at[0, 0], XY)
    S[c, 0, xp] = (S[c, 0, xp].astype(F32) + XR[0, 0].astype(F32)).astype(BF)
    copy(S.at[c, 0, xp], XR.at[0, 2], XP, XY + 4).start()
    got(XR.at[1, 0], XY + 1)
    S[c, 1, xm] = (S[c, 1, xm].astype(F32) + XR[1, 0].astype(F32)).astype(BF)
    copy(S.at[c, 1, xm], XR.at[1, 2], XM, XY + 5).start()

    yfinal(1 - first)

    @pl.when(p < 2)
    def _():
        both(8, lambda k: chain_a(order(k)))

    @pl.when(p >= 2)
    def _():
        both(8, lambda k: chain_b(order(k)))

    got(XR.at[0, 1], XY + 2)
    got(XR.at[1, 1], XY + 3)
    got(XR.at[0, 2], XY + 4)
    got(XR.at[1, 2], XY + 5)
    for half, (d0, k0), (d1, k1) in ((0, (0, 2), (1, 1)), (1, (0, 1), (1, 2))):
        ig_out[:, half * 1024 : (half + 1) * 1024] = (
            S[c, half, x].astype(F32) + XR[d0, k0].astype(F32) + XR[d1, k1].astype(F32)
        ).astype(BF)

    @pl.when(p == 0)
    def _():
        for w in range(2):
            FX[w] = G[0, w, y, x]

    @pl.when(p != 0)
    def _():
        for w in range(2):
            got(FX.at[w], FS + w)

    ug_out[...] = FX[0].astype(F32).T * factor
    dg_out[...] = FX[1].astype(F32) * factor

    @pl.when(p != 0)
    def _():
        for w in range(2):
            sent(WS.at[w], SX + w * 4 + x)

    def sends(k):
        w, j = k // 4, k % 4
        piece = wpiece(0, w, y, j)
        sent(piece, ZP + k)

        @pl.when(p != 1)
        def _():
            sent(piece, ZM + k)

        for slot in range(2):
            sent(wpiece(slot, w, y, j), YP + slot * 8 + k)
            sent(wpiece(slot, w, y, j), YM + slot * 8 + k)
        sent(ZA.at[k], GA + k)

        @pl.when(p != 0)
        def _():
            sent(ZB.at[k], GB + k)

        @pl.when((p == 0) & (j != x))
        def _():
            sent(FX.at[w], FSS + k)

        both(2, lambda slot: sent(G.at[slot, w, y, j], GC + slot * 8 + k))
        sent(xblock(w, x, crow), TC + k)

    both(8, sends)
    for i in range(4):
        sent(wblock(0, 0, y), YF + i)
    for i in range(6):
        sent(xblock(0, x, crow), TP + i)
    for i in range(8):
        sent(G.at[0, 0, y], GY + i)
    for i in range(2):
        sent(S.at[0, 0], XC + i)
    for i in range(6):
        sent(S.at[0, 0, 0], XY + i)


def solution(mesh):
    def shards(tokens, up_weight, down_weight, cotangent):
        count_all = tokens.shape[0] * lax.axis_size("fs") * lax.axis_size("tp")
        factor = 1.0 / float(count_all) ** 0.5
        vmem = pl.BlockSpec(memory_space=pltpu.VMEM)
        hbm = pl.BlockSpec(memory_space=pl.ANY)

        def body(*refs):
            kernel(factor, *refs)

        return pl.pallas_call(
            body,
            out_shape=(
                jax.ShapeDtypeStruct((128, 2048), BF),
                jax.ShapeDtypeStruct((128, 256), F32),
                jax.ShapeDtypeStruct((256, 128), F32),
            ),
            in_specs=[hbm, vmem, vmem, hbm],
            out_specs=(vmem, vmem, vmem),
            scratch_shapes=[
                pltpu.VMEM((2, 4, 256, 2048), BF),
                pltpu.VMEM((2, 128, 256), BF),
                pltpu.VMEM((2, 2, 2048, 256), BF),
                pltpu.VMEM((2, 1024, 256), BF),
                pltpu.VMEM((2, 2, 256, 1024), BF),
                pltpu.VMEM((2, 2, 4, 4, 256, 128), BF),
                pltpu.VMEM((2, 2, 2, 4, 256, 128), BF),
                pltpu.VMEM((2, 2, 4, 256, 128), BF),
                pltpu.VMEM((8, 256, 128), BF),
                pltpu.VMEM((8, 256, 128), BF),
                pltpu.VMEM((2, 256, 128), BF),
                pltpu.VMEM((2, 2, 4, 128, 1024), BF),
                pltpu.VMEM((2, 4, 128, 1024), BF),
                pltpu.VMEM((2, 3, 128, 1024), BF),
                pltpu.SemaphoreType.DMA((N_SEM,)),
                pltpu.SemaphoreType.DMA((N_SEM,)),
                pltpu.SemaphoreType.DMA((2,)),
            ],
            compiler_params=pltpu.CompilerParams(
                collective_id=0, has_side_effects=True, vmem_limit_bytes=60 * 2**20
            ),
            name="ffn_backward",
        )(tokens, up_weight, down_weight, cotangent)

    placed = (P(("fs", "tp"), None), P("fs", "tp"), P("tp", "fs"), P(("fs", "tp"), None))
    return jax.shard_map(
        shards,
        mesh=mesh,
        in_specs=placed,
        out_specs=(P(("fs", "tp"), None), P("fs", "tp"), P("tp", "fs")),
        check_vma=False,
    )
```

```python
import jax
import jax.numpy as jnp
from jax import lax
from jax.experimental import pallas as pl
from jax.experimental.pallas import tpu as pltpu
from jax.sharding import PartitionSpec as P

BF = jnp.bfloat16
F32 = jnp.float32
MESH = pl.DeviceIdType.MESH

SX, ZP, ZM, YP, YM, YF = 0, 8, 22, 36, 52, 68
TP, TM, TF, TC = 84, 86, 88, 90
GY, GC, GA, GB, QA, QB, RS = 98, 106, 118, 124, 130, 138, 146
FS, FSS, XC, XY = 152, 154, 162, 164
N_SEM = 170


def both(n, body):
    def step(i, carry):
        body(i)
        return carry

    lax.fori_loop(0, n, step, 0)


def kernel(
    factor, tok_in, up_in, dn_in, cot_in, ig_out, ug_out, dg_out,
    X, WS, W, DP, TT, G, RY, RC, ZA, ZB, UA, UB, RG, FX, S, RP, XR, ssem, rsem, lsem,
):
    fs, tp = lax.axis_index("fs"), lax.axis_index("tp")
    y, x = fs // 4, fs % 4
    z, c = tp // 2, tp % 2
    p = lax.rem(z - x + 8, 4)
    xp, xm, xo = (x + 1) % 4, (x + 3) % 4, (x + 2) % 4
    yp, ym, yo = (y + 1) % 4, (y + 3) % 4, (y + 2) % 4
    zp, zm = (z + 1) % 8, (z + 7) % 8

    def dev(yy, xx, zz, cc):
        return (yy * 4 + xx, zz * 2 + cc)

    XP, XM, XO = dev(y, xp, z, c), dev(y, xm, z, c), dev(y, xo, z, c)
    YPd, YMd = dev(yp, x, z, c), dev(ym, x, z, c)
    ZPd, ZMd = dev(y, x, zp, c), dev(y, x, zm, c)
    PA = dev(y, x, z, 1 - c)

    def copy(src, dst, to, sid, sent_id=None):
        sent_id = sid if sent_id is None else sent_id
        return pltpu.make_async_remote_copy(
            src_ref=src, dst_ref=dst, send_sem=ssem.at[sent_id], recv_sem=rsem.at[sid],
            device_id=to, device_id_type=MESH,
        )

    def got(ref, sid):
        copy(ref, ref, PA, sid).wait_recv()

    def sent(ref, sid):
        copy(ref, ref, PA, sid).wait_send()

    crow = pl.ds(pl.multiple_of(c * 128, 128), 128)
    own = [pltpu.make_async_copy(a, X.at[w, x, crow, :], lsem.at[w]) for w, a in enumerate((tok_in, cot_in))]
    for o in own:
        o.start()
    WS[0] = up_in[...]
    WS[1] = dn_in[...].astype(F32).T.astype(BF)

    barrier = pltpu.get_barrier_semaphore()
    for to in (XP, XM, XO, YPd, YMd, ZPd, ZMd, PA):
        pl.semaphore_signal(barrier, inc=1, device_id=to, device_id_type=MESH)
    pl.semaphore_wait(barrier, 8)

    def wrow(yy, j):
        return pl.ds(pl.multiple_of(yy * 512 + j * 128, 128), 128)

    def wpiece(slot, w, yy, j):
        return W.at[slot, w, wrow(yy, j), :]

    @pl.when(p != 0)
    def _():
        for w in range(2):
            copy(WS.at[w], wpiece(0, w, y, x), dev(y, (x + p) % 4, z, c), SX + w * 4 + x).start()

    for o in own:
        o.wait()

    def xblock(w, xx, cc_row):
        return X.at[w, xx, cc_row, :]

    for w, to, base in ((0, XP, TP), (1, XM, TM), (1, XP, TP), (0, XM, TM)):
        copy(xblock(w, x, crow), xblock(w, x, crow), to, base + w).start()
    for w in range(2):
        copy(xblock(w, x, crow), xblock(w, x, crow), PA, TC + w * 4).start()

    def ysend(slot, w, j):
        piece = wpiece(slot, w, y, j)
        copy(piece, piece, YPd, YP + slot * 8 + w * 4 + j).start()
        copy(piece, piece, YMd, YM + slot * 8 + w * 4 + j).start()

    @pl.when(p == 0)
    def _():
        for w in range(2):
            W[0, w, wrow(y, x), :] = WS[w]
            ysend(0, w, x)

    def root_forward():
        got(wpiece(0, 0, ym, x), YP + x)
        copy(wpiece(0, 0, ym, x), wpiece(0, 0, ym, x), YPd, YF + x).start()
        got(wpiece(0, 1, yp, x), YM + 4 + x)
        copy(wpiece(0, 1, yp, x), wpiece(0, 1, yp, x), YMd, YF + 4 + x).start()

    def root_rest():
        got(wpiece(0, 0, yp, x), YM + x)
        got(wpiece(0, 1, ym, x), YP + 4 + x)
        for w in range(2):
            got(wpiece(0, w, yo, x), YF + w * 4 + x)

    def place(m):
        w, i = m % 2, m // 2
        return w, jnp.where(m < 6, y, (y + i + 1) % 4), jnp.where(m < 6, (x + i + 1) % 4, x)

    def step_a(m):
        w, yy, j = place(m)
        piece = wpiece(0, w, yy, j)

        @pl.when((p == 0) & (m < 6))
        def _():
            got(piece, SX + w * 4 + j)

        @pl.when(p != 0)
        def _():
            got(piece, ZP + m)

        copy(piece, wpiece(jnp.where(p == 3, 1, 0), w, yy, j), ZPd, ZP + m).start()

        @pl.when(p == 0)
        def _():
            copy(piece, wpiece(1, w, yy, j), ZMd, ZM + m).start()

        @pl.when(m < 6)
        def _():
            ysend(0, w, j)

    def step_b(m):
        w, yy, j = place(m)
        piece = wpiece(1, w, yy, j)

        @pl.when(p == 0)
        def _():
            got(piece, ZP + m)

        @pl.when(p != 0)
        def _():
            got(piece, ZM + m)

        @pl.when(p >= 2)
        def _():
            copy(piece, piece, ZMd, ZM + m).start()

        @pl.when(m < 6)
        def _():
            ysend(1, w, j)

    def yforward(slot, m):
        w, j = m % 2, (x + m // 2 + 1) % 4

        @pl.when(w == 0)
        def _():
            piece = wpiece(slot, 0, ym, j)
            got(piece, YP + slot * 8 + j)
            copy(piece, piece, YPd, YF + slot * 8 + j).start()

        @pl.when(w == 1)
        def _():
            piece = wpiece(slot, 1, yp, j)
            got(piece, YM + slot * 8 + 4 + j)
            copy(piece, piece, YMd, YF + slot * 8 + 4 + j).start()

    def pass_on(w, r):
        xx = (x + r) % 4
        copy(xblock(w, xx, crow), xblock(w, xx, crow), PA, TC + w * 4 + r).start()

    near = jnp.where(p < 2, 0, 1)
    far = 1 - near
    root = p == 0
    lag_a = jnp.where(p == 3, 5, 0)
    lag_b = jnp.where(root, 20, jnp.where(p == 1, 5, 0))
    lag_far = jnp.where(root, 28, jnp.where(p == 2, 8, 13))

    def zstep(t):
        @pl.when(root & (t == 2))
        def _():
            root_forward()

        @pl.when(root & (t == 6))
        def _():
            root_rest()

        @pl.when((t >= lag_a) & (t < lag_a + 14))
        def _():
            step_a(t - lag_a)

        @pl.when((t >= lag_b) & (t < lag_b + 14))
        def _():
            step_b(t - lag_b)

        @pl.when(t == jnp.where(root, 14, 6))
        def _():
            got(xblock(0, xm, crow), TP)
            copy(xblock(0, xm, crow), xblock(0, xm, crow), XP, TF).start()
            got(xblock(1, xp, crow), TM + 1)
            copy(xblock(1, xp, crow), xblock(1, xp, crow), XM, TF + 1).start()
            pass_on(0, 3)
            pass_on(1, 1)

        @pl.when(root & (t >= 14) & (t < 20))
        def _():
            yforward(near, t - 14)

        @pl.when((p != 0) & (t >= 4) & (t < 16) & (t % 2 == 0))
        def _():
            yforward(near, (t - 4) // 2)

        @pl.when((t >= lag_far) & (t < lag_far + 6))
        def _():
            yforward(far, t - lag_far)

        @pl.when(t == jnp.where(root, 26, 13))
        def _():
            got(xblock(1, xm, crow), TP + 1)
            pass_on(1, 3)
            got(xblock(0, xp, crow), TM)
            pass_on(0, 1)

    both(34, zstep)

    def yfinish(slot):
        def piece(i):
            j = (x + i + 1) % 4
            got(wpiece(slot, 0, yp, j), YM + slot * 8 + j)
            got(wpiece(slot, 1, ym, j), YP + slot * 8 + 4 + j)
            for w in range(2):
                got(wpiece(slot, w, yo, j), YF + slot * 8 + w * 4 + j)

        both(3, piece)

    orow = pl.ds(pl.multiple_of((1 - c) * 128, 128), 128)

    def partner(r):
        for w in range(2):
            got(xblock(w, (x + r) % 4, orow), TC + w * 4 + r)

    def act(slot, r):
        xx = (x + r) % 4
        pre = jnp.dot(X[0, xx], W[slot, 0], preferred_element_type=F32)
        dh = jnp.dot(X[1, xx], W[slot, 1], preferred_element_type=F32)
        active = jnp.maximum(pre, 0.0)
        hidden = active * active
        dpre = 2.0 * active * dh
        DP[slot, pl.ds(pl.multiple_of(xx * 256, 256), 256), :] = dpre.astype(BF)
        cols = pl.ds(pl.multiple_of(xx * 256, 256), 256)
        TT[slot, 0, :, cols] = dpre.T.astype(BF)
        TT[slot, 1, :, cols] = hidden.T.astype(BF)

    def act_three(slot):
        both(3, lambda i: act(slot, jnp.where(i == 2, 3, i)))

    yfinish(near)
    partner(0)
    partner(1)
    partner(3)
    act_three(near)
    got(xblock(0, xo, crow), TF)
    pass_on(0, 2)
    got(xblock(1, xo, crow), TF + 1)
    pass_on(1, 2)
    yfinish(far)
    act_three(far)
    partner(2)

    def grads(slot, send):
        def block(i):
            yy = (y + jnp.where(i < 2, 2 - i, i + 1)) % 4
            cols = pl.ds(pl.multiple_of(yy * 512, 512), 512)
            for w in range(2):
                rows = X[w, :, :, cols].reshape(1024, 512)
                part = jnp.dot(TT[slot, w], rows, preferred_element_type=F32).astype(BF)
                for j in range(4):
                    G[slot, w, yy, (j - x + 4) % 4] = part[:, j * 128 : (j + 1) * 128]
            if send:
                for at in range(3):

                    @pl.when(i == at)
                    def _(at=at):
                        ab(slot, at)

        both(4, block)

    rest = pl.ds(1, 3)

    def ab(slot, at):
        base = GY + slot * 4
        if at == 0:
            copy(G.at[slot, 0, yo, rest], RY.at[slot, 0, 0], YPd, base).start()
            copy(G.at[slot, 1, yo, rest], RY.at[slot, 1, 0], YMd, base + 1).start()
        if at == 1:
            copy(G.at[slot, 1, yp, rest], RY.at[slot, 0, 1], YPd, base + 2).start()
        if at == 2:
            copy(G.at[slot, 0, ym, rest], RY.at[slot, 1, 1], YMd, base + 3).start()

    def add(*terms):
        total = terms[0].astype(F32)
        for term in terms[1:]:
            total = total + term.astype(F32)
        return total.astype(BF)

    def cstep(slot):
        base = GY + slot * 4
        got(RY.at[slot, 0, 0], base)
        got(RY.at[slot, 1, 0], base + 1)

        def piece(i):
            G[slot, 0, yp, i + 1] = add(G[slot, 0, yp, i + 1], RY[slot, 0, 0, i])
            copy(G.at[slot, 0, yp, i + 1], RC.at[slot, 0, i], YPd, GC + slot * 6 + i).start()
            G[slot, 1, ym, i + 1] = add(G[slot, 1, ym, i + 1], RY[slot, 1, 0, i])
            copy(G.at[slot, 1, ym, i + 1], RC.at[slot, 1, i], YMd, GC + slot * 6 + 3 + i).start()

        both(3, piece)

    def chain_b(m):
        w, i = m % 2, m // 2 + 1

        @pl.when(root)
        def _():
            copy(G.at[1, w, y, i], ZA.at[m], ZMd, GA + m).start()

        @pl.when(p >= 2)
        def _():
            got(ZB.at[m], GB + m)
            G[1, w, y, i] = add(G[1, w, y, i], ZB[m])

        @pl.when(p != 0)
        def _():
            copy(G.at[1, w, y, i], ZB.at[m], ZPd, GB + m).start()

    def chain_a(m):
        w, i = m % 2, m // 2 + 1
        got(ZA.at[m], GA + m)

        @pl.when(p != 0)
        def _():
            G[0, w, y, i] = add(G[0, w, y, i], ZA[m])
            copy(G.at[0, w, y, i], ZA.at[m], ZMd, GA + m).start()

        @pl.when(root)
        def _():
            got(ZB.at[m], GB + m)
            G[0, w, y, i] = add(G[0, w, y, i], ZA[m], ZB[m])
            copy(G.at[0, w, y, i], FX.at[w], dev(y, (x + i) % 4, z, c), FS + w, FSS + w * 4 + i).start()

    def yfinal(slot, after):
        base = GY + slot * 4
        got(RY.at[slot, 0, 1], base + 2)
        got(RY.at[slot, 1, 1], base + 3)

        def piece(i):
            got(RC.at[slot, 0, i], GC + slot * 6 + i)
            G[slot, 0, y, i + 1] = add(G[slot, 0, y, i + 1], RC[slot, 0, i], RY[slot, 1, 1, i])
            got(RC.at[slot, 1, i], GC + slot * 6 + 3 + i)
            G[slot, 1, y, i + 1] = add(G[slot, 1, y, i + 1], RC[slot, 1, i], RY[slot, 0, 1, i])
            after(i)

        both(3, piece)

    def qplace(q):
        i = q // 2
        return q % 2, (y + jnp.where(i < 2, 2 - i, i + 1)) % 4

    def own_b(q):
        w, yy = qplace(q)

        @pl.when(root)
        def _():
            copy(G.at[1, w, yy, 0], UA.at[q], ZMd, QA + q).start()

        @pl.when(p >= 2)
        def _():
            got(UB.at[q], QB + q)
            G[1, w, yy, 0] = add(G[1, w, yy, 0], UB[q])

        @pl.when(p != 0)
        def _():
            copy(G.at[1, w, yy, 0], UB.at[q], ZPd, QB + q).start()

    def own_a(q):
        w, yy = qplace(q)
        got(UA.at[q], QA + q)

        @pl.when(p != 0)
        def _():
            G[0, w, yy, 0] = add(G[0, w, yy, 0], UA[q])
            copy(G.at[0, w, yy, 0], UA.at[q], ZMd, QA + q).start()

        @pl.when(root)
        def _():
            got(UB.at[q], QB + q)
            G[0, w, yy, 0] = add(G[0, w, yy, 0], UA[q], UB[q])

            @pl.when(q == 0)
            def _():
                copy(G.at[0, 0, yo, 0], RG.at[0, 0], YPd, RS).start()

            @pl.when(q == 1)
            def _():
                copy(G.at[0, 1, yo, 0], RG.at[1, 0], YMd, RS + 1).start()

            @pl.when(q == 3)
            def _():
                copy(G.at[0, 1, yp, 0], RG.at[0, 1], YPd, RS + 2).start()

            @pl.when(q == 4)
            def _():
                copy(G.at[0, 0, ym, 0], RG.at[1, 1], YMd, RS + 3).start()

    def igrad(n):
        rows = pl.ds(pl.multiple_of(n * 256, 256), 256)
        nt = (((1,), (1,)), ((), ()))
        part = lax.dot_general(DP[0], W[0, 0, rows, :], nt, preferred_element_type=F32)
        part = part + lax.dot_general(DP[1], W[1, 0, rows, :], nt, preferred_element_type=F32)
        part = part.astype(BF).reshape(4, 2, 128, 256)
        cols = pl.ds(pl.multiple_of((n % 4) * 256, 256), 256)
        for cc in range(2):
            S[cc, n // 4, :, :, cols] = part[:, cc]

    act(far, 2)
    grads(far, True)

    @pl.when(p < 2)
    def _():
        both(8, own_b)

    act(near, 2)
    grads(near, False)
    cstep(far)
    for at in range(3):
        ab(near, at)
    for half in range(2):
        both(4, lambda n, half=half: igrad(half * 4 + n))
        copy(S.at[1 - c, half], RP.at[half], PA, XC + half).start()

    for half in range(2):
        got(RP.at[half], XC + half)

        def xadd(r, half=half):
            S[c, half, r] = add(S[c, half, r], RP[half, r])

        both(4, xadd)
    copy(S.at[c, 0, xo], XR.at[0, 0], XP, XY).start()
    copy(S.at[c, 1, xo], XR.at[1, 0], XM, XY + 1).start()
    copy(S.at[c, 1, xp], XR.at[0, 1], XP, XY + 2).start()
    copy(S.at[c, 0, xm], XR.at[1, 1], XM, XY + 3).start()

    @pl.when(p >= 2)
    def _():
        both(8, own_a)

    def head(i):
        @pl.when(p < 2)
        def _():
            chain_b(i * 2)
            chain_b(i * 2 + 1)

    yfinal(far, head)
    cstep(near)

    @pl.when(p == 1)
    def _():
        both(8, own_a)

    @pl.when(p == 2)
    def _():
        both(8, own_b)

    @pl.when(p >= 2)
    def _():
        both(6, chain_a)

    @pl.when(p == 3)
    def _():
        both(8, own_b)

    got(XR.at[0, 0], XY)
    S[c, 0, xp] = add(S[c, 0, xp], XR[0, 0])
    copy(S.at[c, 0, xp], XR.at[0, 2], XP, XY + 4).start()
    got(XR.at[1, 0], XY + 1)
    S[c, 1, xm] = add(S[c, 1, xm], XR[1, 0])
    copy(S.at[c, 1, xm], XR.at[1, 2], XM, XY + 5).start()

    def tail(i):
        @pl.when(p == 1)
        def _():
            chain_a(i * 2)
            chain_a(i * 2 + 1)

        @pl.when(p >= 2)
        def _():
            chain_b(i * 2)
            chain_b(i * 2 + 1)

    yfinal(near, tail)

    @pl.when(root)
    def _():
        both(8, own_a)
        both(6, chain_a)
        got(RG.at[0, 0], RS)
        G[0, 0, yp, 0] = add(G[0, 0, yp, 0], RG[0, 0])
        copy(G.at[0, 0, yp, 0], RG.at[0, 2], YPd, RS + 4).start()
        got(RG.at[1, 0], RS + 1)
        G[0, 1, ym, 0] = add(G[0, 1, ym, 0], RG[1, 0])
        copy(G.at[0, 1, ym, 0], RG.at[1, 2], YMd, RS + 5).start()

    got(XR.at[0, 1], XY + 2)
    got(XR.at[1, 1], XY + 3)
    got(XR.at[0, 2], XY + 4)
    got(XR.at[1, 2], XY + 5)
    for half, (d0, k0), (d1, k1) in ((0, (0, 2), (1, 1)), (1, (0, 1), (1, 2))):
        ig_out[:, half * 1024 : (half + 1) * 1024] = add(S[c, half, x], XR[d0, k0], XR[d1, k1])

    @pl.when(root)
    def _():
        for k in range(1, 5):
            got(RG.at[(k + 1) % 2, (k + 1) // 2], RS + k + 1)
        FX[0] = add(G[0, 0, y, 0], RG[0, 2], RG[1, 1])
        FX[1] = add(G[0, 1, y, 0], RG[0, 1], RG[1, 2])

    @pl.when(p != 0)
    def _():
        for w in range(2):
            got(FX.at[w], FS + w)

    ug_out[...] = FX[0].astype(F32).T * factor
    dg_out[...] = FX[1].astype(F32) * factor

    unit = FX.at[0]

    @pl.when(p != 0)
    def _():
        for w in range(2):
            sent(unit, SX + w * 4 + x)

    def chain_sends(m):
        sent(unit, ZP + m)

        @pl.when(p != 1)
        def _():
            sent(unit, ZM + m)

    both(14, chain_sends)

    def sends(k):
        w, j = k // 4, k % 4
        for slot in range(2):

            @pl.when((j != x) | (root & (slot == 0)))
            def _(slot=slot):
                for base in (YP, YM, YF):
                    sent(unit, base + slot * 8 + k)

        sent(UA.at[k], QA + k)

        @pl.when(p != 0)
        def _():
            sent(UB.at[k], QB + k)

        @pl.when(root & (j != 0))
        def _():
            sent(unit, FSS + k)

        sent(xblock(w, x, crow), TC + k)
        sent(RY.at[0, 0, 0], GY + k)

    both(8, sends)

    def more_sends(m):
        sent(unit, GC + m)
        sent(unit, GC + 6 + m)
        sent(unit, GA + m)

        @pl.when(p != 0)
        def _():
            sent(unit, GB + m)

        @pl.when(root)
        def _():
            sent(unit, RS + m)

        sent(xblock(0, x, crow), TP + m)
        sent(XR.at[0, 0], XY + m)

    both(6, more_sends)
    for i in range(2):
        sent(RP.at[0], XC + i)


def solution(mesh):
    def shards(tokens, up_weight, down_weight, cotangent):
        count_all = tokens.shape[0] * lax.axis_size("fs") * lax.axis_size("tp")
        factor = 1.0 / float(count_all) ** 0.5
        vmem = pl.BlockSpec(memory_space=pltpu.VMEM)
        hbm = pl.BlockSpec(memory_space=pl.ANY)

        def body(*refs):
            kernel(factor, *refs)

        return pl.pallas_call(
            body,
            out_shape=(
                jax.ShapeDtypeStruct((128, 2048), BF),
                jax.ShapeDtypeStruct((128, 256), F32),
                jax.ShapeDtypeStruct((256, 128), F32),
            ),
            in_specs=[hbm, vmem, vmem, hbm],
            out_specs=(vmem, vmem, vmem),
            scratch_shapes=[
                pltpu.VMEM((2, 4, 256, 2048), BF),
                pltpu.VMEM((2, 128, 256), BF),
                pltpu.VMEM((2, 2, 2048, 256), BF),
                pltpu.VMEM((2, 1024, 256), BF),
                pltpu.VMEM((2, 2, 256, 1024), BF),
                pltpu.VMEM((2, 2, 4, 4, 256, 128), BF),
                pltpu.VMEM((2, 2, 2, 3, 256, 128), BF),
                pltpu.VMEM((2, 2, 3, 256, 128), BF),
                pltpu.VMEM((6, 256, 128), BF),
                pltpu.VMEM((6, 256, 128), BF),
                pltpu.VMEM((8, 256, 128), BF),
                pltpu.VMEM((8, 256, 128), BF),
                pltpu.VMEM((2, 3, 256, 128), BF),
                pltpu.VMEM((2, 256, 128), BF),
                pltpu.VMEM((2, 2, 4, 128, 1024), BF),
                pltpu.VMEM((2, 4, 128, 1024), BF),
                pltpu.VMEM((2, 3, 128, 1024), BF),
                pltpu.SemaphoreType.DMA((N_SEM,)),
                pltpu.SemaphoreType.DMA((N_SEM,)),
                pltpu.SemaphoreType.DMA((2,)),
            ],
            compiler_params=pltpu.CompilerParams(
                collective_id=0, has_side_effects=True, vmem_limit_bytes=60 * 2**20
            ),
            name="ffn_backward",
        )(tokens, up_weight, down_weight, cotangent)

    placed = (P(("fs", "tp"), None), P("fs", "tp"), P("tp", "fs"), P(("fs", "tp"), None))
    return jax.shard_map(
        shards,
        mesh=mesh,
        in_specs=placed,
        out_specs=(P(("fs", "tp"), None), P("fs", "tp"), P("tp", "fs")),
        check_vma=False,
    )
```

```python
import jax
import jax.numpy as jnp
from jax import lax
from jax.experimental import pallas as pl
from jax.experimental.pallas import tpu as pltpu
from jax.sharding import PartitionSpec as P

BF = jnp.bfloat16
F32 = jnp.float32
MESH = pl.DeviceIdType.MESH

SX, ZP, ZM, YP, YM, YF = 0, 8, 22, 36, 52, 68
TP, TM, TF, TC = 84, 86, 88, 90
AY, BY, GC, GA, GB, QA, QB, RS = 98, 110, 122, 134, 140, 146, 154, 162
FS, FSS, XC, XY = 168, 170, 178, 180
N_SEM = 186


def both(n, body):
    def step(i, carry):
        body(i)
        return carry

    lax.fori_loop(0, n, step, 0)


def kernel(
    factor, tok_in, up_in, dn_in, cot_in, ig_out, ug_out, dg_out,
    X, WS, W, DP, TT, G, RY, RC, ZA, ZB, UA, UB, RG, FX, S, RP, XR, ssem, rsem, lsem,
):
    fs, tp = lax.axis_index("fs"), lax.axis_index("tp")
    y, x = fs // 4, fs % 4
    z, c = tp // 2, tp % 2
    p = lax.rem(z - x + 8, 4)
    xp, xm, xo = (x + 1) % 4, (x + 3) % 4, (x + 2) % 4
    yp, ym, yo = (y + 1) % 4, (y + 3) % 4, (y + 2) % 4
    zp, zm = (z + 1) % 8, (z + 7) % 8

    def dev(yy, xx, zz, cc):
        return (yy * 4 + xx, zz * 2 + cc)

    XP, XM, XO = dev(y, xp, z, c), dev(y, xm, z, c), dev(y, xo, z, c)
    YPd, YMd = dev(yp, x, z, c), dev(ym, x, z, c)
    ZPd, ZMd = dev(y, x, zp, c), dev(y, x, zm, c)
    PA = dev(y, x, z, 1 - c)

    def copy(src, dst, to, sid, sent_id=None):
        sent_id = sid if sent_id is None else sent_id
        return pltpu.make_async_remote_copy(
            src_ref=src, dst_ref=dst, send_sem=ssem.at[sent_id], recv_sem=rsem.at[sid],
            device_id=to, device_id_type=MESH,
        )

    def got(ref, sid):
        copy(ref, ref, PA, sid).wait_recv()

    def sent(ref, sid):
        copy(ref, ref, PA, sid).wait_send()

    crow = pl.ds(pl.multiple_of(c * 128, 128), 128)
    own = [pltpu.make_async_copy(a, X.at[w, x, crow, :], lsem.at[w]) for w, a in enumerate((tok_in, cot_in))]
    for o in own:
        o.start()
    WS[0] = up_in[...]
    WS[1] = dn_in[...].astype(F32).T.astype(BF)

    barrier = pltpu.get_barrier_semaphore()
    for to in (XP, XM, XO, YPd, YMd, ZPd, ZMd, PA):
        pl.semaphore_signal(barrier, inc=1, device_id=to, device_id_type=MESH)
    pl.semaphore_wait(barrier, 8)

    def wrow(yy, j):
        return pl.ds(pl.multiple_of(yy * 512 + j * 128, 128), 128)

    def wpiece(slot, w, yy, j):
        return W.at[slot, w, wrow(yy, j), :]

    @pl.when(p != 0)
    def _():
        for w in range(2):
            copy(WS.at[w], wpiece(0, w, y, x), dev(y, (x + p) % 4, z, c), SX + w * 4 + x).start()

    for o in own:
        o.wait()

    def xblock(w, xx, cc_row):
        return X.at[w, xx, cc_row, :]

    for w, to, base in ((0, XP, TP), (1, XM, TM), (1, XP, TP), (0, XM, TM)):
        copy(xblock(w, x, crow), xblock(w, x, crow), to, base + w).start()
    for w in range(2):
        copy(xblock(w, x, crow), xblock(w, x, crow), PA, TC + w * 4).start()

    def ysend(slot, w, j):
        piece = wpiece(slot, w, y, j)
        copy(piece, piece, YPd, YP + slot * 8 + w * 4 + j).start()
        copy(piece, piece, YMd, YM + slot * 8 + w * 4 + j).start()

    @pl.when(p == 0)
    def _():
        for w in range(2):
            W[0, w, wrow(y, x), :] = WS[w]
            ysend(0, w, x)

    def root_forward():
        got(wpiece(0, 0, ym, x), YP + x)
        copy(wpiece(0, 0, ym, x), wpiece(0, 0, ym, x), YPd, YF + x).start()
        got(wpiece(0, 1, yp, x), YM + 4 + x)
        copy(wpiece(0, 1, yp, x), wpiece(0, 1, yp, x), YMd, YF + 4 + x).start()

    def root_rest():
        got(wpiece(0, 0, yp, x), YM + x)
        got(wpiece(0, 1, ym, x), YP + 4 + x)
        for w in range(2):
            got(wpiece(0, w, yo, x), YF + w * 4 + x)

    def place(m):
        w, i = m % 2, m // 2
        return w, jnp.where(m < 6, y, (y + i + 1) % 4), jnp.where(m < 6, (x + i + 1) % 4, x)

    def step_a(m):
        w, yy, j = place(m)
        piece = wpiece(0, w, yy, j)

        @pl.when((p == 0) & (m < 6))
        def _():
            got(piece, SX + w * 4 + j)

        @pl.when(p != 0)
        def _():
            got(piece, ZP + m)

        copy(piece, wpiece(jnp.where(p == 3, 1, 0), w, yy, j), ZPd, ZP + m).start()

        @pl.when(p == 0)
        def _():
            copy(piece, wpiece(1, w, yy, j), ZMd, ZM + m).start()

        @pl.when(m < 6)
        def _():
            ysend(0, w, j)

    def step_b(m):
        w, yy, j = place(m)
        piece = wpiece(1, w, yy, j)

        @pl.when(p == 0)
        def _():
            got(piece, ZP + m)

        @pl.when(p != 0)
        def _():
            got(piece, ZM + m)

        @pl.when(p >= 2)
        def _():
            copy(piece, piece, ZMd, ZM + m).start()

        @pl.when(m < 6)
        def _():
            ysend(1, w, j)

    def yforward(slot, m):
        w, j = m % 2, (x + m // 2 + 1) % 4

        @pl.when(w == 0)
        def _():
            piece = wpiece(slot, 0, ym, j)
            got(piece, YP + slot * 8 + j)
            copy(piece, piece, YPd, YF + slot * 8 + j).start()

        @pl.when(w == 1)
        def _():
            piece = wpiece(slot, 1, yp, j)
            got(piece, YM + slot * 8 + 4 + j)
            copy(piece, piece, YMd, YF + slot * 8 + 4 + j).start()

    def pass_on(w, r):
        xx = (x + r) % 4
        copy(xblock(w, xx, crow), xblock(w, xx, crow), PA, TC + w * 4 + r).start()

    near = jnp.where(p < 2, 0, 1)
    far = 1 - near
    root = p == 0
    lag_a = jnp.where(p == 3, 5, 0)
    lag_b = jnp.where(root, 20, jnp.where(p == 1, 5, 0))
    lag_far = jnp.where(root, 28, jnp.where(p == 2, 8, 13))

    def yfinish(slot):
        def piece(i):
            j = (x + i + 1) % 4
            got(wpiece(slot, 0, yp, j), YM + slot * 8 + j)
            got(wpiece(slot, 1, ym, j), YP + slot * 8 + 4 + j)
            for w in range(2):
                got(wpiece(slot, w, yo, j), YF + slot * 8 + w * 4 + j)

        both(3, piece)

    orow = pl.ds(pl.multiple_of((1 - c) * 128, 128), 128)

    def partner(r):
        for w in range(2):
            got(xblock(w, (x + r) % 4, orow), TC + w * 4 + r)

    def act(slot, r):
        xx = (x + r) % 4
        pre = jnp.dot(X[0, xx], W[slot, 0], preferred_element_type=F32)
        dh = jnp.dot(X[1, xx], W[slot, 1], preferred_element_type=F32)
        active = jnp.maximum(pre, 0.0)
        hidden = active * active
        dpre = 2.0 * active * dh
        DP[slot, pl.ds(pl.multiple_of(xx * 256, 256), 256), :] = dpre.astype(BF)
        cols = pl.ds(pl.multiple_of(xx * 256, 256), 256)
        TT[slot, 0, :, cols] = dpre.T.astype(BF)
        TT[slot, 1, :, cols] = hidden.T.astype(BF)

    def act_three(slot):
        both(3, lambda i: act(slot, jnp.where(i == 2, 3, i)))

    def near_part():
        yfinish(near)
        partner(0)
        partner(1)
        partner(3)
        act_three(near)

    def zstep(t):
        @pl.when(root & (t == 2))
        def _():
            root_forward()

        @pl.when(root & (t == 6))
        def _():
            root_rest()

        @pl.when((t >= lag_a) & (t < lag_a + 14))
        def _():
            step_a(t - lag_a)

        @pl.when((t >= lag_b) & (t < lag_b + 14))
        def _():
            step_b(t - lag_b)

        @pl.when(t == jnp.where(root, 14, 6))
        def _():
            got(xblock(0, xm, crow), TP)
            copy(xblock(0, xm, crow), xblock(0, xm, crow), XP, TF).start()
            got(xblock(1, xp, crow), TM + 1)
            copy(xblock(1, xp, crow), xblock(1, xp, crow), XM, TF + 1).start()
            pass_on(0, 3)
            pass_on(1, 1)

        @pl.when(root & (t >= 14) & (t < 20))
        def _():
            yforward(near, t - 14)

        @pl.when((p != 0) & (t >= 4) & (t < 16) & (t % 2 == 0))
        def _():
            yforward(near, (t - 4) // 2)

        @pl.when((t >= lag_far) & (t < lag_far + 6))
        def _():
            yforward(far, t - lag_far)

        @pl.when(t == jnp.where(root, 26, 13))
        def _():
            got(xblock(1, xm, crow), TP + 1)
            pass_on(1, 3)
            got(xblock(0, xp, crow), TM)
            pass_on(0, 1)

        @pl.when(root & (t == 27))
        def _():
            near_part()

    both(34, zstep)

    pl.when(p != 0)(near_part)
    got(xblock(0, xo, crow), TF)
    pass_on(0, 2)
    got(xblock(1, xo, crow), TF + 1)
    pass_on(1, 2)
    yfinish(far)
    act_three(far)
    partner(2)

    def grads(slot, send):
        def block(i):
            yy = (y + jnp.where(i < 2, 2 - i, i + 1)) % 4
            cols = pl.ds(pl.multiple_of(yy * 512, 512), 512)
            for w in range(2):
                rows = X[w, :, :, cols].reshape(1024, 512)
                part = jnp.dot(TT[slot, w], rows, preferred_element_type=F32).astype(BF)
                for j in range(4):
                    G[slot, w, yy, (j - x + 4) % 4] = part[:, j * 128 : (j + 1) * 128]
            if send:
                for at, copies in enumerate((a_send, bp_send, bm_send)):

                    @pl.when(i == at)
                    def _(copies=copies):
                        both(3, lambda n: copies(slot, n))

        both(4, block)

    def a_send(slot, i):
        copy(G.at[slot, 0, yo, i + 1], RY.at[slot, 0, 0, i], YPd, AY + slot * 6 + i).start()
        copy(G.at[slot, 1, yo, i + 1], RY.at[slot, 1, 0, i], YMd, AY + slot * 6 + 3 + i).start()

    def bp_send(slot, i):
        copy(G.at[slot, 1, yp, i + 1], RY.at[slot, 0, 1, i], YPd, BY + slot * 6 + i).start()

    def bm_send(slot, i):
        copy(G.at[slot, 0, ym, i + 1], RY.at[slot, 1, 1, i], YMd, BY + slot * 6 + 3 + i).start()

    def ab_send(slot, i):
        a_send(slot, i)
        bp_send(slot, i)
        bm_send(slot, i)

    def add(*terms):
        total = terms[0].astype(F32)
        for term in terms[1:]:
            total = total + term.astype(F32)
        return total.astype(BF)

    def c_step(slot, i):
        got(RY.at[slot, 0, 0, i], AY + slot * 6 + i)
        G[slot, 0, yp, i + 1] = add(G[slot, 0, yp, i + 1], RY[slot, 0, 0, i])
        copy(G.at[slot, 0, yp, i + 1], RC.at[slot, 0, i], YPd, GC + slot * 6 + i).start()
        got(RY.at[slot, 1, 0, i], AY + slot * 6 + 3 + i)
        G[slot, 1, ym, i + 1] = add(G[slot, 1, ym, i + 1], RY[slot, 1, 0, i])
        copy(G.at[slot, 1, ym, i + 1], RC.at[slot, 1, i], YMd, GC + slot * 6 + 3 + i).start()

    def chain_b(m):
        w, i = m % 2, m // 2 + 1

        @pl.when(root)
        def _():
            copy(G.at[1, w, y, i], ZA.at[m], ZMd, GA + m).start()

        @pl.when(p >= 2)
        def _():
            got(ZB.at[m], GB + m)
            G[1, w, y, i] = add(G[1, w, y, i], ZB[m])

        @pl.when(p != 0)
        def _():
            copy(G.at[1, w, y, i], ZB.at[m], ZPd, GB + m).start()

    def chain_a(m):
        w, i = m % 2, m // 2 + 1
        got(ZA.at[m], GA + m)

        @pl.when(p != 0)
        def _():
            G[0, w, y, i] = add(G[0, w, y, i], ZA[m])
            copy(G.at[0, w, y, i], ZA.at[m], ZMd, GA + m).start()

        @pl.when(root)
        def _():
            got(ZB.at[m], GB + m)
            G[0, w, y, i] = add(G[0, w, y, i], ZA[m], ZB[m])
            copy(G.at[0, w, y, i], FX.at[w], dev(y, (x + i) % 4, z, c), FS + w, FSS + w * 4 + i).start()

    def y_final(slot, i):
        got(RY.at[slot, 1, 1, i], BY + slot * 6 + 3 + i)
        got(RC.at[slot, 0, i], GC + slot * 6 + i)
        G[slot, 0, y, i + 1] = add(G[slot, 0, y, i + 1], RC[slot, 0, i], RY[slot, 1, 1, i])
        got(RY.at[slot, 0, 1, i], BY + slot * 6 + i)
        got(RC.at[slot, 1, i], GC + slot * 6 + 3 + i)
        G[slot, 1, y, i + 1] = add(G[slot, 1, y, i + 1], RC[slot, 1, i], RY[slot, 0, 1, i])

    def qplace(q):
        i = q // 2
        return q % 2, (y + jnp.where(i < 2, 2 - i, i + 1)) % 4

    def own_b(q):
        w, yy = qplace(q)

        @pl.when(root)
        def _():
            copy(G.at[1, w, yy, 0], UA.at[q], ZMd, QA + q).start()

        @pl.when(p >= 2)
        def _():
            got(UB.at[q], QB + q)
            G[1, w, yy, 0] = add(G[1, w, yy, 0], UB[q])

        @pl.when(p != 0)
        def _():
            copy(G.at[1, w, yy, 0], UB.at[q], ZPd, QB + q).start()

    def own_a(q):
        w, yy = qplace(q)
        got(UA.at[q], QA + q)

        @pl.when(p != 0)
        def _():
            G[0, w, yy, 0] = add(G[0, w, yy, 0], UA[q])
            copy(G.at[0, w, yy, 0], UA.at[q], ZMd, QA + q).start()

        @pl.when(root)
        def _():
            got(UB.at[q], QB + q)
            G[0, w, yy, 0] = add(G[0, w, yy, 0], UA[q], UB[q])

            @pl.when(q == 0)
            def _():
                copy(G.at[0, 0, yo, 0], RG.at[0, 0], YPd, RS).start()

            @pl.when(q == 1)
            def _():
                copy(G.at[0, 1, yo, 0], RG.at[1, 0], YMd, RS + 1).start()

            @pl.when(q == 3)
            def _():
                copy(G.at[0, 1, yp, 0], RG.at[0, 1], YPd, RS + 2).start()

            @pl.when(q == 4)
            def _():
                copy(G.at[0, 0, ym, 0], RG.at[1, 1], YMd, RS + 3).start()

    def igrad(n):
        rows = pl.ds(pl.multiple_of(n * 256, 256), 256)
        nt = (((1,), (1,)), ((), ()))
        part = lax.dot_general(DP[0], W[0, 0, rows, :], nt, preferred_element_type=F32)
        part = part + lax.dot_general(DP[1], W[1, 0, rows, :], nt, preferred_element_type=F32)
        part = part.astype(BF).reshape(4, 2, 128, 256)
        cols = pl.ds(pl.multiple_of((n % 4) * 256, 256), 256)
        for cc in range(2):
            S[cc, n // 4, :, :, cols] = part[:, cc]

    act(far, 2)
    grads(far, True)

    @pl.when(p < 2)
    def _():
        both(8, own_b)

    act(near, 2)
    grads(near, False)
    both(3, lambda i: c_step(far, i))
    both(2, lambda i: ab_send(near, i))

    def x_first(half):
        got(RP.at[half], XC + half)
        both(4, lambda r: xadd(half, r))

    def xadd(half, r):
        S[c, half, r] = add(S[c, half, r], RP[half, r])

    def x_send():
        copy(S.at[c, 0, xo], XR.at[0, 0], XP, XY).start()
        copy(S.at[c, 1, xo], XR.at[1, 0], XM, XY + 1).start()
        copy(S.at[c, 1, xp], XR.at[0, 1], XP, XY + 2).start()
        copy(S.at[c, 0, xm], XR.at[1, 1], XM, XY + 3).start()

    def x_second():
        got(XR.at[0, 0], XY)
        S[c, 0, xp] = add(S[c, 0, xp], XR[0, 0])
        copy(S.at[c, 0, xp], XR.at[0, 2], XP, XY + 4).start()
        got(XR.at[1, 0], XY + 1)
        S[c, 1, xm] = add(S[c, 1, xm], XR[1, 0])
        copy(S.at[c, 1, xm], XR.at[1, 2], XM, XY + 5).start()

    def root_second():
        got(RG.at[0, 0], RS)
        G[0, 0, yp, 0] = add(G[0, 0, yp, 0], RG[0, 0])
        copy(G.at[0, 0, yp, 0], RG.at[0, 2], YPd, RS + 4).start()
        got(RG.at[1, 0], RS + 1)
        G[0, 1, ym, 0] = add(G[0, 1, ym, 0], RG[1, 0])
        copy(G.at[0, 1, ym, 0], RG.at[1, 2], YMd, RS + 5).start()

    def by_p(*values):
        return jnp.where(p == 0, values[0], jnp.where(p == 1, values[1], jnp.where(p == 2, values[2], values[3])))

    never = 99
    at_own_b = by_p(never, never, 1, 3)
    at_own_a = by_p(12, 9, 6, 3)
    at_chain_a = by_p(20, 18, 13, 10)
    at_chain_b = by_p(never, never, never, 18)

    def rstep(t):
        def span(start, count, body):
            @pl.when((t >= start) & (t < start + count))
            def _():
                body(t - start)

        span(at_own_b, 8, own_b)
        span(at_own_a, 8, own_a)
        span(at_chain_b, 6, chain_b)

        @pl.when(root & (t == 20))
        def _():
            root_second()

        span(at_chain_a, 6, chain_a)

        @pl.when(t < 4)
        def _():
            igrad(t * 2)
            igrad(t * 2 + 1)

        @pl.when((t == 1) | (t == 3))
        def _():
            half = t // 2
            copy(S.at[1 - c, half], RP.at[half], PA, XC + half).start()

        @pl.when((t == 5) | (t == 6))
        def _():
            x_first(t - 5)

        @pl.when(t == 6)
        def _():
            x_send()

        @pl.when(t == 8)
        def _():
            def piece(i):
                y_final(far, i)

                @pl.when(p < 2)
                def _():
                    chain_b(i * 2)
                    chain_b(i * 2 + 1)

            both(3, piece)

        span(9, 2, lambda i: c_step(near, i))

        @pl.when(t == 10)
        def _():
            ab_send(near, 2)

        @pl.when(t == 12)
        def _():
            x_second()

        @pl.when(t == 14)
        def _():
            c_step(near, 2)

        @pl.when((t == 13) | (t == 15) | (t == 17))
        def _():
            i = (t - 13) // 2
            y_final(near, i)

            @pl.when(p == 2)
            def _():
                chain_b(i * 2)
                chain_b(i * 2 + 1)

    both(26, rstep)

    got(XR.at[0, 1], XY + 2)
    got(XR.at[1, 1], XY + 3)
    got(XR.at[0, 2], XY + 4)
    got(XR.at[1, 2], XY + 5)
    for half, (d0, k0), (d1, k1) in ((0, (0, 2), (1, 1)), (1, (0, 1), (1, 2))):
        ig_out[:, half * 1024 : (half + 1) * 1024] = add(S[c, half, x], XR[d0, k0], XR[d1, k1])

    @pl.when(root)
    def _():
        for k in range(1, 5):
            got(RG.at[(k + 1) % 2, (k + 1) // 2], RS + k + 1)
        FX[0] = add(G[0, 0, y, 0], RG[0, 2], RG[1, 1])
        FX[1] = add(G[0, 1, y, 0], RG[0, 1], RG[1, 2])

    @pl.when(p != 0)
    def _():
        for w in range(2):
            got(FX.at[w], FS + w)

    ug_out[...] = FX[0].astype(F32).T * factor
    dg_out[...] = FX[1].astype(F32) * factor

    unit = FX.at[0]

    @pl.when(p != 0)
    def _():
        for w in range(2):
            sent(unit, SX + w * 4 + x)

    def chain_sends(m):
        sent(unit, ZP + m)

        @pl.when(p != 1)
        def _():
            sent(unit, ZM + m)

    both(14, chain_sends)

    def sends(k):
        w, j = k // 4, k % 4
        for slot in range(2):

            @pl.when((j != x) | (root & (slot == 0)))
            def _(slot=slot):
                for base in (YP, YM, YF):
                    sent(unit, base + slot * 8 + k)

        sent(UA.at[k], QA + k)

        @pl.when(p != 0)
        def _():
            sent(UB.at[k], QB + k)

        @pl.when(root & (j != 0))
        def _():
            sent(unit, FSS + k)

        sent(xblock(w, x, crow), TC + k)

    both(8, sends)

    def more_sends(m):
        sent(unit, GC + m)
        sent(unit, GC + 6 + m)
        for base in (AY, BY):
            sent(unit, base + m)
            sent(unit, base + 6 + m)
        sent(unit, GA + m)

        @pl.when(p != 0)
        def _():
            sent(unit, GB + m)

        @pl.when(root)
        def _():
            sent(unit, RS + m)

        sent(xblock(0, x, crow), TP + m)
        sent(XR.at[0, 0], XY + m)

    both(6, more_sends)
    for i in range(2):
        sent(RP.at[0], XC + i)


def solution(mesh):
    def shards(tokens, up_weight, down_weight, cotangent):
        count_all = tokens.shape[0] * lax.axis_size("fs") * lax.axis_size("tp")
        factor = 1.0 / float(count_all) ** 0.5
        vmem = pl.BlockSpec(memory_space=pltpu.VMEM)
        hbm = pl.BlockSpec(memory_space=pl.ANY)

        def body(*refs):
            kernel(factor, *refs)

        return pl.pallas_call(
            body,
            out_shape=(
                jax.ShapeDtypeStruct((128, 2048), BF),
                jax.ShapeDtypeStruct((128, 256), F32),
                jax.ShapeDtypeStruct((256, 128), F32),
            ),
            in_specs=[hbm, vmem, vmem, hbm],
            out_specs=(vmem, vmem, vmem),
            scratch_shapes=[
                pltpu.VMEM((2, 4, 256, 2048), BF),
                pltpu.VMEM((2, 128, 256), BF),
                pltpu.VMEM((2, 2, 2048, 256), BF),
                pltpu.VMEM((2, 1024, 256), BF),
                pltpu.VMEM((2, 2, 256, 1024), BF),
                pltpu.VMEM((2, 2, 4, 4, 256, 128), BF),
                pltpu.VMEM((2, 2, 2, 3, 256, 128), BF),
                pltpu.VMEM((2, 2, 3, 256, 128), BF),
                pltpu.VMEM((6, 256, 128), BF),
                pltpu.VMEM((6, 256, 128), BF),
                pltpu.VMEM((8, 256, 128), BF),
                pltpu.VMEM((8, 256, 128), BF),
                pltpu.VMEM((2, 3, 256, 128), BF),
                pltpu.VMEM((2, 256, 128), BF),
                pltpu.VMEM((2, 2, 4, 128, 1024), BF),
                pltpu.VMEM((2, 4, 128, 1024), BF),
                pltpu.VMEM((2, 3, 128, 1024), BF),
                pltpu.SemaphoreType.DMA((N_SEM,)),
                pltpu.SemaphoreType.DMA((N_SEM,)),
                pltpu.SemaphoreType.DMA((2,)),
            ],
            compiler_params=pltpu.CompilerParams(
                collective_id=0, has_side_effects=True, vmem_limit_bytes=60 * 2**20
            ),
            name="ffn_backward",
        )(tokens, up_weight, down_weight, cotangent)

    placed = (P(("fs", "tp"), None), P("fs", "tp"), P("tp", "fs"), P(("fs", "tp"), None))
    return jax.shard_map(
        shards,
        mesh=mesh,
        in_specs=placed,
        out_specs=(P(("fs", "tp"), None), P("fs", "tp"), P("tp", "fs")),
        check_vma=False,
    )
```

```python
import jax
import jax.numpy as jnp
from jax import lax
from jax.experimental import pallas as pl
from jax.experimental.pallas import tpu as pltpu
from jax.sharding import PartitionSpec as P

BF = jnp.bfloat16
F32 = jnp.float32
MESH = pl.DeviceIdType.MESH

SX, ZP, ZM, YP, YM, YF = 0, 8, 22, 36, 52, 68
TP, TM, TF, TC = 84, 86, 88, 90
AY, BY, GC, GA, GB, QA, QB, RS = 98, 110, 122, 134, 140, 146, 154, 162
FS, FSS, XC, XY = 168, 170, 178, 180
N_SEM = 186


def both(n, body):
    def step(i, carry):
        body(i)
        return carry

    lax.fori_loop(0, n, step, 0)


def kernel(
    factor, tok_in, up_in, dn_in, cot_in, ig_out, ug_out, dg_out,
    X, WS, W, DP, TT, G, RY, RC, ZA, ZB, UA, UB, RG, FX, S, RP, XR, ssem, rsem, lsem,
):
    fs, tp = lax.axis_index("fs"), lax.axis_index("tp")
    y, x = fs // 4, fs % 4
    z, c = tp // 2, tp % 2
    p = lax.rem(z - x + 8, 4)
    xp, xm, xo = (x + 1) % 4, (x + 3) % 4, (x + 2) % 4
    yp, ym, yo = (y + 1) % 4, (y + 3) % 4, (y + 2) % 4
    zp, zm = (z + 1) % 8, (z + 7) % 8

    def dev(yy, xx, zz, cc):
        return (yy * 4 + xx, zz * 2 + cc)

    XP, XM, XO = dev(y, xp, z, c), dev(y, xm, z, c), dev(y, xo, z, c)
    YPd, YMd = dev(yp, x, z, c), dev(ym, x, z, c)
    ZPd, ZMd = dev(y, x, zp, c), dev(y, x, zm, c)
    PA = dev(y, x, z, 1 - c)

    def copy(src, dst, to, sid, sent_id=None):
        sent_id = sid if sent_id is None else sent_id
        return pltpu.make_async_remote_copy(
            src_ref=src, dst_ref=dst, send_sem=ssem.at[sent_id], recv_sem=rsem.at[sid],
            device_id=to, device_id_type=MESH,
        )

    def got(ref, sid):
        copy(ref, ref, PA, sid).wait_recv()

    def sent(ref, sid):
        copy(ref, ref, PA, sid).wait_send()

    crow = pl.ds(pl.multiple_of(c * 128, 128), 128)
    own = [pltpu.make_async_copy(a, X.at[w, x, crow, :], lsem.at[w]) for w, a in enumerate((tok_in, cot_in))]
    for o in own:
        o.start()
    WS[0] = up_in[...]
    WS[1] = dn_in[...].astype(F32).T.astype(BF)

    barrier = pltpu.get_barrier_semaphore()
    for to in (XP, XM, XO, YPd, YMd, ZPd, ZMd, PA):
        pl.semaphore_signal(barrier, inc=1, device_id=to, device_id_type=MESH)
    pl.semaphore_wait(barrier, 8)

    def wrow(yy, j):
        return pl.ds(pl.multiple_of(yy * 512 + j * 128, 128), 128)

    def wpiece(slot, w, yy, j):
        return W.at[slot, w, wrow(yy, j), :]

    @pl.when(p != 0)
    def _():
        for w in range(2):
            copy(WS.at[w], wpiece(0, w, y, x), dev(y, (x + p) % 4, z, c), SX + w * 4 + x).start()

    for o in own:
        o.wait()

    def xblock(w, xx, cc_row):
        return X.at[w, xx, cc_row, :]

    for w, to, base in ((0, XP, TP), (1, XM, TM), (1, XP, TP), (0, XM, TM)):
        copy(xblock(w, x, crow), xblock(w, x, crow), to, base + w).start()
    for w in range(2):
        copy(xblock(w, x, crow), xblock(w, x, crow), PA, TC + w * 4).start()

    def ysend(slot, w, j):
        piece = wpiece(slot, w, y, j)
        copy(piece, piece, YPd, YP + slot * 8 + w * 4 + j).start()
        copy(piece, piece, YMd, YM + slot * 8 + w * 4 + j).start()

    @pl.when(p == 0)
    def _():
        for w in range(2):
            W[0, w, wrow(y, x), :] = WS[w]
            ysend(0, w, x)

    def root_forward():
        got(wpiece(0, 0, ym, x), YP + x)
        copy(wpiece(0, 0, ym, x), wpiece(0, 0, ym, x), YPd, YF + x).start()
        got(wpiece(0, 1, yp, x), YM + 4 + x)
        copy(wpiece(0, 1, yp, x), wpiece(0, 1, yp, x), YMd, YF + 4 + x).start()

    def root_rest():
        got(wpiece(0, 0, yp, x), YM + x)
        got(wpiece(0, 1, ym, x), YP + 4 + x)
        for w in range(2):
            got(wpiece(0, w, yo, x), YF + w * 4 + x)

    def place(m):
        w, i = m % 2, m // 2
        return w, jnp.where(i < 4, y, (y + i + 1) % 4), jnp.where(i < 4, (x + i) % 4, x)

    def step_a(m):
        w, yy, j = place(m)
        piece = wpiece(0, w, yy, j)

        @pl.when((p == 0) & (m >= 2) & (m < 8))
        def _():
            got(piece, SX + w * 4 + j)

        @pl.when(p != 0)
        def _():
            got(piece, ZP + m)

        copy(piece, wpiece(jnp.where(p == 3, 1, 0), w, yy, j), ZPd, ZP + m).start()

        @pl.when(p == 0)
        def _():
            copy(piece, wpiece(1, w, yy, j), ZMd, ZM + m).start()

        @pl.when((m >= 2) & (m < 8))
        def _():
            ysend(0, w, j)

    def step_b(m):
        w, yy, j = place(m)
        piece = wpiece(1, w, yy, j)

        @pl.when(p == 0)
        def _():
            got(piece, ZP + m)

        @pl.when(p != 0)
        def _():
            got(piece, ZM + m)

        @pl.when(p >= 2)
        def _():
            copy(piece, piece, ZMd, ZM + m).start()

        @pl.when((m >= 2) & (m < 8))
        def _():
            ysend(1, w, j)

    def yforward(slot, m):
        w, j = m % 2, (x + m // 2 + 1) % 4

        @pl.when(w == 0)
        def _():
            piece = wpiece(slot, 0, ym, j)
            got(piece, YP + slot * 8 + j)
            copy(piece, piece, YPd, YF + slot * 8 + j).start()

        @pl.when(w == 1)
        def _():
            piece = wpiece(slot, 1, yp, j)
            got(piece, YM + slot * 8 + 4 + j)
            copy(piece, piece, YMd, YF + slot * 8 + 4 + j).start()

    def pass_on(w, r):
        xx = (x + r) % 4
        copy(xblock(w, xx, crow), xblock(w, xx, crow), PA, TC + w * 4 + r).start()

    near = jnp.where(p < 2, 0, 1)
    far = 1 - near
    root = p == 0
    lag_a = jnp.where(p == 3, 5, 0)
    lag_b = jnp.where(root, 20, jnp.where(p == 1, 5, 0))
    lag_far = jnp.where(root, 28, jnp.where(p == 2, 10, 15))

    def yfinish(slot):
        def piece(i):
            j = (x + i + 1) % 4
            got(wpiece(slot, 0, yp, j), YM + slot * 8 + j)
            got(wpiece(slot, 1, ym, j), YP + slot * 8 + 4 + j)
            for w in range(2):
                got(wpiece(slot, w, yo, j), YF + slot * 8 + w * 4 + j)

        both(3, piece)

    orow = pl.ds(pl.multiple_of((1 - c) * 128, 128), 128)

    def partner(r):
        for w in range(2):
            got(xblock(w, (x + r) % 4, orow), TC + w * 4 + r)

    def act(slot, r):
        xx = (x + r) % 4
        pre = jnp.dot(X[0, xx], W[slot, 0], preferred_element_type=F32)
        dh = jnp.dot(X[1, xx], W[slot, 1], preferred_element_type=F32)
        active = jnp.maximum(pre, 0.0)
        hidden = active * active
        dpre = 2.0 * active * dh
        DP[slot, pl.ds(pl.multiple_of(xx * 256, 256), 256), :] = dpre.astype(BF)
        cols = pl.ds(pl.multiple_of(xx * 256, 256), 256)
        TT[slot, 0, :, cols] = dpre.T.astype(BF)
        TT[slot, 1, :, cols] = hidden.T.astype(BF)

    def act_three(slot):
        both(3, lambda i: act(slot, jnp.where(i == 2, 3, i)))

    def near_part():
        yfinish(near)
        partner(0)
        partner(1)
        partner(3)
        act_three(near)

    def zstep(t):
        @pl.when(root & (t == 2))
        def _():
            root_forward()

        @pl.when(root & (t == 6))
        def _():
            root_rest()

        @pl.when((t >= lag_a) & (t < lag_a + 14))
        def _():
            step_a(t - lag_a)

        @pl.when((t >= lag_b) & (t < lag_b + 14))
        def _():
            step_b(t - lag_b)

        @pl.when(t == jnp.where(root, 14, 8))
        def _():
            got(xblock(0, xm, crow), TP)
            copy(xblock(0, xm, crow), xblock(0, xm, crow), XP, TF).start()
            got(xblock(1, xp, crow), TM + 1)
            copy(xblock(1, xp, crow), xblock(1, xp, crow), XM, TF + 1).start()
            pass_on(0, 3)
            pass_on(1, 1)

        @pl.when(root & (t >= 14) & (t < 20))
        def _():
            yforward(near, t - 14)

        @pl.when((p != 0) & (t >= 6) & (t < 18) & (t % 2 == 0))
        def _():
            yforward(near, (t - 6) // 2)

        @pl.when((t >= lag_far) & (t < lag_far + 6))
        def _():
            yforward(far, t - lag_far)

        @pl.when(t == jnp.where(root, 26, 15))
        def _():
            got(xblock(1, xm, crow), TP + 1)
            pass_on(1, 3)
            got(xblock(0, xp, crow), TM)
            pass_on(0, 1)

        @pl.when(root & (t == 27))
        def _():
            near_part()

    both(34, zstep)

    pl.when(p != 0)(near_part)
    got(xblock(0, xo, crow), TF)
    pass_on(0, 2)
    got(xblock(1, xo, crow), TF + 1)
    pass_on(1, 2)
    yfinish(far)
    act_three(far)
    partner(2)

    def grads(slot, send, first=0, count=4):
        def block(i):
            yy = (y + jnp.where(i < 2, 2 - i, i + 1)) % 4
            cols = pl.ds(pl.multiple_of(yy * 512, 512), 512)
            for w in range(2):
                rows = X[w, :, :, cols].reshape(1024, 512)
                part = jnp.dot(TT[slot, w], rows, preferred_element_type=F32).astype(BF)
                for j in range(4):
                    G[slot, w, yy, (j - x + 4) % 4] = part[:, j * 128 : (j + 1) * 128]
            if send:

                @pl.when(i == 0)
                def _():
                    both(3, lambda n: a_send(slot, n))

                @pl.when(p < 2)
                def _():
                    own_b(2 * i)
                    own_b(2 * i + 1)

        both(count, lambda i: block(first + i))

    def a_send(slot, i):
        copy(G.at[slot, 0, yo, i + 1], RY.at[slot, 0, 0, i], YPd, AY + slot * 6 + i).start()
        copy(G.at[slot, 1, yo, i + 1], RY.at[slot, 1, 0, i], YMd, AY + slot * 6 + 3 + i).start()

    def b_send(slot, i):
        copy(G.at[slot, 1, yp, i + 1], RY.at[slot, 0, 1, i], YPd, BY + slot * 6 + i).start()
        copy(G.at[slot, 0, ym, i + 1], RY.at[slot, 1, 1, i], YMd, BY + slot * 6 + 3 + i).start()

    def add(*terms):
        total = terms[0].astype(F32)
        for term in terms[1:]:
            total = total + term.astype(F32)
        return total.astype(BF)

    def c_step(slot, i):
        got(RY.at[slot, 0, 0, i], AY + slot * 6 + i)
        G[slot, 0, yp, i + 1] = add(G[slot, 0, yp, i + 1], RY[slot, 0, 0, i])
        copy(G.at[slot, 0, yp, i + 1], RC.at[slot, 0, i], YPd, GC + slot * 6 + i).start()
        got(RY.at[slot, 1, 0, i], AY + slot * 6 + 3 + i)
        G[slot, 1, ym, i + 1] = add(G[slot, 1, ym, i + 1], RY[slot, 1, 0, i])
        copy(G.at[slot, 1, ym, i + 1], RC.at[slot, 1, i], YMd, GC + slot * 6 + 3 + i).start()

    def chain_b(m):
        w, i = m % 2, m // 2 + 1

        @pl.when(root)
        def _():
            copy(G.at[1, w, y, i], ZA.at[m], ZMd, GA + m).start()

        @pl.when(p >= 2)
        def _():
            got(ZB.at[m], GB + m)
            G[1, w, y, i] = add(G[1, w, y, i], ZB[m])

        @pl.when(p != 0)
        def _():
            copy(G.at[1, w, y, i], ZB.at[m], ZPd, GB + m).start()

    def chain_a(m):
        w, i = m % 2, m // 2 + 1
        got(ZA.at[m], GA + m)

        @pl.when(p != 0)
        def _():
            G[0, w, y, i] = add(G[0, w, y, i], ZA[m])
            copy(G.at[0, w, y, i], ZA.at[m], ZMd, GA + m).start()

        @pl.when(root)
        def _():
            got(ZB.at[m], GB + m)
            G[0, w, y, i] = add(G[0, w, y, i], ZA[m], ZB[m])
            copy(G.at[0, w, y, i], FX.at[w], dev(y, (x + i) % 4, z, c), FS + w, FSS + w * 4 + i).start()

    def y_final(slot, i):
        got(RY.at[slot, 1, 1, i], BY + slot * 6 + 3 + i)
        got(RC.at[slot, 0, i], GC + slot * 6 + i)
        G[slot, 0, y, i + 1] = add(G[slot, 0, y, i + 1], RC[slot, 0, i], RY[slot, 1, 1, i])
        got(RY.at[slot, 0, 1, i], BY + slot * 6 + i)
        got(RC.at[slot, 1, i], GC + slot * 6 + 3 + i)
        G[slot, 1, y, i + 1] = add(G[slot, 1, y, i + 1], RC[slot, 1, i], RY[slot, 0, 1, i])

    def qplace(q):
        i = q // 2
        return q % 2, (y + jnp.where(i < 2, 2 - i, i + 1)) % 4

    def own_b(q):
        w, yy = qplace(q)

        @pl.when(root)
        def _():
            copy(G.at[1, w, yy, 0], UA.at[q], ZMd, QA + q).start()

        @pl.when(p >= 2)
        def _():
            got(UB.at[q], QB + q)
            G[1, w, yy, 0] = add(G[1, w, yy, 0], UB[q])

        @pl.when(p != 0)
        def _():
            copy(G.at[1, w, yy, 0], UB.at[q], ZPd, QB + q).start()

    def own_a(q):
        w, yy = qplace(q)
        got(UA.at[q], QA + q)

        @pl.when(p != 0)
        def _():
            G[0, w, yy, 0] = add(G[0, w, yy, 0], UA[q])
            copy(G.at[0, w, yy, 0], UA.at[q], ZMd, QA + q).start()

        @pl.when(root)
        def _():
            got(UB.at[q], QB + q)
            G[0, w, yy, 0] = add(G[0, w, yy, 0], UA[q], UB[q])

            @pl.when(q == 0)
            def _():
                copy(G.at[0, 0, yo, 0], RG.at[0, 0], YPd, RS).start()

            @pl.when(q == 1)
            def _():
                copy(G.at[0, 1, yo, 0], RG.at[1, 0], YMd, RS + 1).start()

            @pl.when(q == 3)
            def _():
                copy(G.at[0, 1, yp, 0], RG.at[0, 1], YPd, RS + 2).start()

            @pl.when(q == 4)
            def _():
                copy(G.at[0, 0, ym, 0], RG.at[1, 1], YMd, RS + 3).start()

    def igrad(n):
        rows = pl.ds(pl.multiple_of(n * 256, 256), 256)
        nt = (((1,), (1,)), ((), ()))
        part = lax.dot_general(DP[0], W[0, 0, rows, :], nt, preferred_element_type=F32)
        part = part + lax.dot_general(DP[1], W[1, 0, rows, :], nt, preferred_element_type=F32)
        part = part.astype(BF).reshape(4, 2, 128, 256)
        cols = pl.ds(pl.multiple_of((n % 4) * 256, 256), 256)
        for cc in range(2):
            S[cc, n // 4, :, :, cols] = part[:, cc]

    act(far, 2)
    grads(far, True)

    b_send(far, 0)
    act(near, 2)
    c_step(far, 0)
    b_send(far, 1)
    grads(near, False, 0, 2)
    c_step(far, 1)
    b_send(far, 2)
    grads(near, False, 2, 2)
    c_step(far, 2)
    both(3, lambda i: a_send(near, i))
    b_send(near, 0)

    def x_first(half):
        got(RP.at[half], XC + half)
        both(4, lambda r: xadd(half, r))

    def xadd(half, r):
        S[c, half, r] = add(S[c, half, r], RP[half, r])

    def x_send():
        copy(S.at[c, 0, xo], XR.at[0, 0], XP, XY).start()
        copy(S.at[c, 1, xo], XR.at[1, 0], XM, XY + 1).start()
        copy(S.at[c, 1, xp], XR.at[0, 1], XP, XY + 2).start()
        copy(S.at[c, 0, xm], XR.at[1, 1], XM, XY + 3).start()

    def x_second():
        got(XR.at[0, 0], XY)
        S[c, 0, xp] = add(S[c, 0, xp], XR[0, 0])
        copy(S.at[c, 0, xp], XR.at[0, 2], XP, XY + 4).start()
        got(XR.at[1, 0], XY + 1)
        S[c, 1, xm] = add(S[c, 1, xm], XR[1, 0])
        copy(S.at[c, 1, xm], XR.at[1, 2], XM, XY + 5).start()

    def root_second():
        got(RG.at[0, 0], RS)
        G[0, 0, yp, 0] = add(G[0, 0, yp, 0], RG[0, 0])
        copy(G.at[0, 0, yp, 0], RG.at[0, 2], YPd, RS + 4).start()
        got(RG.at[1, 0], RS + 1)
        G[0, 1, ym, 0] = add(G[0, 1, ym, 0], RG[1, 0])
        copy(G.at[0, 1, ym, 0], RG.at[1, 2], YMd, RS + 5).start()

    def by_p(*values):
        return jnp.where(p == 0, values[0], jnp.where(p == 1, values[1], jnp.where(p == 2, values[2], values[3])))

    never = 99
    at_own_b = by_p(never, never, 0, 3)
    at_own_a = by_p(10, 7, 4, 1)
    at_chain_a = by_p(18, 15, 12, 9)
    at_chain_b = by_p(never, never, never, 15)

    def rstep(t):
        def span(start, count, body):
            @pl.when((t >= start) & (t < start + count))
            def _():
                body(t - start)

        span(at_own_b, 8, own_b)
        span(at_own_a, 8, own_a)
        span(at_chain_b, 6, chain_b)

        @pl.when(root & (t == 18))
        def _():
            root_second()

        span(at_chain_a, 6, chain_a)

        @pl.when(t < 4)
        def _():
            igrad(t * 2)
            igrad(t * 2 + 1)

        @pl.when((t == 1) | (t == 3))
        def _():
            half = t // 2
            copy(S.at[1 - c, half], RP.at[half], PA, XC + half).start()

        @pl.when((t == 4) | (t == 5) | (t == 7))
        def _():
            i = (t - 3) // 2
            y_final(far, i)

            @pl.when(p < 2)
            def _():
                chain_b(i * 2)
                chain_b(i * 2 + 1)

        @pl.when((t == 5) | (t == 6))
        def _():
            x_first(t - 5)

        @pl.when(t == 6)
        def _():
            x_send()

        @pl.when((t >= 8) & (t < 11))
        def _():
            i = t - 8
            c_step(near, i)

            @pl.when(i < 2)
            def _():
                b_send(near, i + 1)

        @pl.when(t == 13)
        def _():
            x_second()

        @pl.when((t == 12) | (t == 14) | (t == 16))
        def _():
            i = (t - 12) // 2
            y_final(near, i)

            @pl.when(p == 2)
            def _():
                chain_b(i * 2)
                chain_b(i * 2 + 1)

    both(24, rstep)

    got(XR.at[0, 1], XY + 2)
    got(XR.at[1, 1], XY + 3)
    got(XR.at[0, 2], XY + 4)
    got(XR.at[1, 2], XY + 5)
    for half, (d0, k0), (d1, k1) in ((0, (0, 2), (1, 1)), (1, (0, 1), (1, 2))):
        ig_out[:, half * 1024 : (half + 1) * 1024] = add(S[c, half, x], XR[d0, k0], XR[d1, k1])

    @pl.when(root)
    def _():
        for k in range(1, 5):
            got(RG.at[(k + 1) % 2, (k + 1) // 2], RS + k + 1)
        FX[0] = add(G[0, 0, y, 0], RG[0, 2], RG[1, 1])
        FX[1] = add(G[0, 1, y, 0], RG[0, 1], RG[1, 2])

    @pl.when(p != 0)
    def _():
        for w in range(2):
            got(FX.at[w], FS + w)

    ug_out[...] = FX[0].astype(F32).T * factor
    dg_out[...] = FX[1].astype(F32) * factor

    unit = FX.at[0]

    @pl.when(p != 0)
    def _():
        for w in range(2):
            sent(unit, SX + w * 4 + x)

    def chain_sends(m):
        sent(unit, ZP + m)

        @pl.when(p != 1)
        def _():
            sent(unit, ZM + m)

    both(14, chain_sends)

    def sends(k):
        w, j = k // 4, k % 4
        for slot in range(2):

            @pl.when((j != x) | (root & (slot == 0)))
            def _(slot=slot):
                for base in (YP, YM, YF):
                    sent(unit, base + slot * 8 + k)

        sent(UA.at[k], QA + k)

        @pl.when(p != 0)
        def _():
            sent(UB.at[k], QB + k)

        @pl.when(root & (j != 0))
        def _():
            sent(unit, FSS + k)

        sent(xblock(w, x, crow), TC + k)

    both(8, sends)

    def more_sends(m):
        sent(unit, GC + m)
        sent(unit, GC + 6 + m)
        for base in (AY, BY):
            sent(unit, base + m)
            sent(unit, base + 6 + m)
        sent(unit, GA + m)

        @pl.when(p != 0)
        def _():
            sent(unit, GB + m)

        @pl.when(root)
        def _():
            sent(unit, RS + m)

        sent(xblock(0, x, crow), TP + m)
        sent(XR.at[0, 0], XY + m)

    both(6, more_sends)
    for i in range(2):
        sent(RP.at[0], XC + i)


def solution(mesh):
    def shards(tokens, up_weight, down_weight, cotangent):
        count_all = tokens.shape[0] * lax.axis_size("fs") * lax.axis_size("tp")
        factor = 1.0 / float(count_all) ** 0.5
        vmem = pl.BlockSpec(memory_space=pltpu.VMEM)
        hbm = pl.BlockSpec(memory_space=pl.ANY)

        def body(*refs):
            kernel(factor, *refs)

        return pl.pallas_call(
            body,
            out_shape=(
                jax.ShapeDtypeStruct((128, 2048), BF),
                jax.ShapeDtypeStruct((128, 256), F32),
                jax.ShapeDtypeStruct((256, 128), F32),
            ),
            in_specs=[hbm, vmem, vmem, hbm],
            out_specs=(vmem, vmem, vmem),
            scratch_shapes=[
                pltpu.VMEM((2, 4, 256, 2048), BF),
                pltpu.VMEM((2, 128, 256), BF),
                pltpu.VMEM((2, 2, 2048, 256), BF),
                pltpu.VMEM((2, 1024, 256), BF),
                pltpu.VMEM((2, 2, 256, 1024), BF),
                pltpu.VMEM((2, 2, 4, 4, 256, 128), BF),
                pltpu.VMEM((2, 2, 2, 3, 256, 128), BF),
                pltpu.VMEM((2, 2, 3, 256, 128), BF),
                pltpu.VMEM((6, 256, 128), BF),
                pltpu.VMEM((6, 256, 128), BF),
                pltpu.VMEM((8, 256, 128), BF),
                pltpu.VMEM((8, 256, 128), BF),
                pltpu.VMEM((2, 3, 256, 128), BF),
                pltpu.VMEM((2, 256, 128), BF),
                pltpu.VMEM((2, 2, 4, 128, 1024), BF),
                pltpu.VMEM((2, 4, 128, 1024), BF),
                pltpu.VMEM((2, 3, 128, 1024), BF),
                pltpu.SemaphoreType.DMA((N_SEM,)),
                pltpu.SemaphoreType.DMA((N_SEM,)),
                pltpu.SemaphoreType.DMA((2,)),
            ],
            compiler_params=pltpu.CompilerParams(
                collective_id=0, has_side_effects=True, vmem_limit_bytes=60 * 2**20
            ),
            name="ffn_backward",
        )(tokens, up_weight, down_weight, cotangent)

    placed = (P(("fs", "tp"), None), P("fs", "tp"), P("tp", "fs"), P(("fs", "tp"), None))
    return jax.shard_map(
        shards,
        mesh=mesh,
        in_specs=placed,
        out_specs=(P(("fs", "tp"), None), P("fs", "tp"), P("tp", "fs")),
        check_vma=False,
    )
```

```python
import jax
import jax.numpy as jnp
from jax import lax
from jax.experimental import pallas as pl
from jax.experimental.pallas import tpu as pltpu
from jax.sharding import PartitionSpec as P

BF = jnp.bfloat16
F32 = jnp.float32
MESH = pl.DeviceIdType.MESH

SX, ZP, ZM, YP, YM, YF = 0, 8, 22, 36, 52, 68
TP, TM, TF, TC = 84, 86, 88, 90
AY, BY, GC, GA, GB, QA, QB, RS = 98, 110, 122, 134, 140, 146, 154, 162
FS, FSS, XC, XY = 168, 170, 178, 180
N_SEM = 186


def both(n, body):
    def step(i, carry):
        body(i)
        return carry

    lax.fori_loop(0, n, step, 0)


def kernel(
    factor, tok_in, up_in, dn_in, cot_in, ig_out, ug_out, dg_out,
    X, WS, W, DP, TT, G, RY, RC, ZA, ZB, UA, UB, RG, FX, S, RP, XR, ssem, rsem, lsem,
):
    fs, tp = lax.axis_index("fs"), lax.axis_index("tp")
    y, x = fs // 4, fs % 4
    z, c = tp // 2, tp % 2
    p = lax.rem(z - x + 8, 4)
    xp, xm, xo = (x + 1) % 4, (x + 3) % 4, (x + 2) % 4
    yp, ym, yo = (y + 1) % 4, (y + 3) % 4, (y + 2) % 4
    zp, zm = (z + 1) % 8, (z + 7) % 8

    def dev(yy, xx, zz, cc):
        return (yy * 4 + xx, zz * 2 + cc)

    XP, XM, XO = dev(y, xp, z, c), dev(y, xm, z, c), dev(y, xo, z, c)
    YPd, YMd = dev(yp, x, z, c), dev(ym, x, z, c)
    ZPd, ZMd = dev(y, x, zp, c), dev(y, x, zm, c)
    PA = dev(y, x, z, 1 - c)

    def copy(src, dst, to, sid, sent_id=None):
        sent_id = sid if sent_id is None else sent_id
        return pltpu.make_async_remote_copy(
            src_ref=src, dst_ref=dst, send_sem=ssem.at[sent_id], recv_sem=rsem.at[sid],
            device_id=to, device_id_type=MESH,
        )

    def got(ref, sid):
        copy(ref, ref, PA, sid).wait_recv()

    def sent(ref, sid):
        copy(ref, ref, PA, sid).wait_send()

    crow = pl.ds(pl.multiple_of(c * 128, 128), 128)
    own = [pltpu.make_async_copy(a, X.at[w, x, crow, :], lsem.at[w]) for w, a in enumerate((tok_in, cot_in))]
    for o in own:
        o.start()
    WS[0] = up_in[...]
    WS[1] = dn_in[...].astype(F32).T.astype(BF)

    barrier = pltpu.get_barrier_semaphore()
    for to in (XP, XM, XO, YPd, YMd, ZPd, ZMd, PA):
        pl.semaphore_signal(barrier, inc=1, device_id=to, device_id_type=MESH)
    pl.semaphore_wait(barrier, 8)

    def wrow(yy, j):
        return pl.ds(pl.multiple_of(yy * 512 + j * 128, 128), 128)

    def wpiece(slot, w, yy, j):
        return W.at[slot, w, wrow(yy, j), :]

    @pl.when(p != 0)
    def _():
        for w in range(2):
            copy(WS.at[w], wpiece(0, w, y, x), dev(y, (x + p) % 4, z, c), SX + w * 4 + x).start()

    for o in own:
        o.wait()

    def xblock(w, xx, cc_row):
        return X.at[w, xx, cc_row, :]

    for w, to, base in ((0, XP, TP), (1, XM, TM), (1, XP, TP), (0, XM, TM)):
        copy(xblock(w, x, crow), xblock(w, x, crow), to, base + w).start()
    for w in range(2):
        copy(xblock(w, x, crow), xblock(w, x, crow), PA, TC + w * 4).start()

    def ysend(slot, w, j):
        piece = wpiece(slot, w, y, j)
        copy(piece, piece, YPd, YP + slot * 8 + w * 4 + j).start()
        copy(piece, piece, YMd, YM + slot * 8 + w * 4 + j).start()

    @pl.when(p == 0)
    def _():
        for w in range(2):
            W[0, w, wrow(y, x), :] = WS[w]
            ysend(0, w, x)

    def root_forward():
        got(wpiece(0, 0, ym, x), YP + x)
        copy(wpiece(0, 0, ym, x), wpiece(0, 0, ym, x), YPd, YF + x).start()
        got(wpiece(0, 1, yp, x), YM + 4 + x)
        copy(wpiece(0, 1, yp, x), wpiece(0, 1, yp, x), YMd, YF + 4 + x).start()

    def root_rest():
        got(wpiece(0, 0, yp, x), YM + x)
        got(wpiece(0, 1, ym, x), YP + 4 + x)
        for w in range(2):
            got(wpiece(0, w, yo, x), YF + w * 4 + x)

    def place(m):
        w, i = m % 2, m // 2
        return w, jnp.where(i < 4, y, (y + i + 1) % 4), jnp.where(i < 4, (x + i) % 4, x)

    def step_a(m):
        w, yy, j = place(m)
        piece = wpiece(0, w, yy, j)

        @pl.when((p == 0) & (m >= 2) & (m < 8))
        def _():
            got(piece, SX + w * 4 + j)

        @pl.when(p != 0)
        def _():
            got(piece, ZP + m)

        copy(piece, wpiece(jnp.where(p == 3, 1, 0), w, yy, j), ZPd, ZP + m).start()

        @pl.when(p == 0)
        def _():
            copy(piece, wpiece(1, w, yy, j), ZMd, ZM + m).start()

        @pl.when((m >= 2) & (m < 8))
        def _():
            ysend(0, w, j)

    def step_b(m):
        w, yy, j = place(m)
        piece = wpiece(1, w, yy, j)

        @pl.when(p == 0)
        def _():
            got(piece, ZP + m)

        @pl.when(p != 0)
        def _():
            got(piece, ZM + m)

        @pl.when(p >= 2)
        def _():
            copy(piece, piece, ZMd, ZM + m).start()

        @pl.when((m >= 2) & (m < 8))
        def _():
            ysend(1, w, j)

    def yforward(slot, m):
        w, j = m % 2, (x + m // 2 + 1) % 4

        @pl.when(w == 0)
        def _():
            piece = wpiece(slot, 0, ym, j)
            got(piece, YP + slot * 8 + j)
            copy(piece, piece, YPd, YF + slot * 8 + j).start()

        @pl.when(w == 1)
        def _():
            piece = wpiece(slot, 1, yp, j)
            got(piece, YM + slot * 8 + 4 + j)
            copy(piece, piece, YMd, YF + slot * 8 + 4 + j).start()

    def pass_on(w, r):
        xx = (x + r) % 4
        copy(xblock(w, xx, crow), xblock(w, xx, crow), PA, TC + w * 4 + r).start()

    near = jnp.where(p < 2, 0, 1)
    far = 1 - near
    root = p == 0
    lag_a = jnp.where(p == 3, 5, 0)
    lag_b = jnp.where(root, 20, jnp.where(p == 1, 5, 0))
    lag_far = jnp.where(root, 28, jnp.where(p == 2, 10, 15))

    def yfinish(slot):
        def piece(i):
            j = (x + i + 1) % 4
            got(wpiece(slot, 0, yp, j), YM + slot * 8 + j)
            got(wpiece(slot, 1, ym, j), YP + slot * 8 + 4 + j)
            for w in range(2):
                got(wpiece(slot, w, yo, j), YF + slot * 8 + w * 4 + j)

        both(3, piece)

    orow = pl.ds(pl.multiple_of((1 - c) * 128, 128), 128)

    def partner(r):
        for w in range(2):
            got(xblock(w, (x + r) % 4, orow), TC + w * 4 + r)

    def act(slot, r):
        xx = (x + r) % 4
        pre = jnp.dot(X[0, xx], W[slot, 0], preferred_element_type=F32)
        dh = jnp.dot(X[1, xx], W[slot, 1], preferred_element_type=F32)
        active = jnp.maximum(pre, 0.0)
        hidden = active * active
        dpre = 2.0 * active * dh
        DP[slot, pl.ds(pl.multiple_of(xx * 256, 256), 256), :] = dpre.astype(BF)
        cols = pl.ds(pl.multiple_of(xx * 256, 256), 256)
        TT[slot, 0, :, cols] = dpre.T.astype(BF)
        TT[slot, 1, :, cols] = hidden.T.astype(BF)

    def act_three(slot):
        both(3, lambda i: act(slot, jnp.where(i == 2, 3, i)))

    def near_part():
        yfinish(near)
        partner(0)
        partner(1)
        partner(3)
        act_three(near)

    def zstep(t):
        @pl.when(root & (t == 2))
        def _():
            root_forward()

        @pl.when(root & (t == 6))
        def _():
            root_rest()

        @pl.when((t >= lag_a) & (t < lag_a + 14))
        def _():
            step_a(t - lag_a)

        @pl.when((t >= lag_b) & (t < lag_b + 14))
        def _():
            step_b(t - lag_b)

        @pl.when(t == jnp.where(root, 14, 8))
        def _():
            got(xblock(0, xm, crow), TP)
            copy(xblock(0, xm, crow), xblock(0, xm, crow), XP, TF).start()
            got(xblock(1, xp, crow), TM + 1)
            copy(xblock(1, xp, crow), xblock(1, xp, crow), XM, TF + 1).start()
            pass_on(0, 3)
            pass_on(1, 1)

        @pl.when(root & (t >= 14) & (t < 20))
        def _():
            yforward(near, t - 14)

        @pl.when((p != 0) & (t >= 6) & (t < 18) & (t % 2 == 0))
        def _():
            yforward(near, (t - 6) // 2)

        @pl.when((t >= lag_far) & (t < lag_far + 6))
        def _():
            yforward(far, t - lag_far)

        @pl.when(t == jnp.where(root, 26, 15))
        def _():
            got(xblock(1, xm, crow), TP + 1)
            pass_on(1, 3)
            got(xblock(0, xp, crow), TM)
            pass_on(0, 1)

        @pl.when(root & (t == 27))
        def _():
            near_part()

    both(34, zstep)

    pl.when(p != 0)(near_part)
    got(xblock(0, xo, crow), TF)
    pass_on(0, 2)
    got(xblock(1, xo, crow), TF + 1)
    pass_on(1, 2)
    yfinish(far)
    act_three(far)
    partner(2)

    def grads(slot, send, first=0, count=4):
        def block(i):
            yy = (y + jnp.where(i < 2, 2 - i, i + 1)) % 4
            cols = pl.ds(pl.multiple_of(yy * 512, 512), 512)
            for w in range(2):
                rows = X[w, :, :, cols].reshape(1024, 512)
                part = jnp.dot(TT[slot, w], rows, preferred_element_type=F32).astype(BF)
                for j in range(4):
                    G[slot, w, yy, (j - x + 4) % 4] = part[:, j * 128 : (j + 1) * 128]
            if send:

                @pl.when(i == 0)
                def _():
                    both(3, lambda n: a_send(slot, n))

                @pl.when(p < 2)
                def _():
                    own_b(2 * i)
                    own_b(2 * i + 1)

        both(count, lambda i: block(first + i))

    def a_send(slot, i):
        copy(G.at[slot, 0, yo, i + 1], RY.at[slot, 0, 0, i], YPd, AY + slot * 6 + i).start()
        copy(G.at[slot, 1, yo, i + 1], RY.at[slot, 1, 0, i], YMd, AY + slot * 6 + 3 + i).start()

    def b_send(slot, i):
        copy(G.at[slot, 1, yp, i + 1], RY.at[slot, 0, 1, i], YPd, BY + slot * 6 + i).start()
        copy(G.at[slot, 0, ym, i + 1], RY.at[slot, 1, 1, i], YMd, BY + slot * 6 + 3 + i).start()

    def add(*terms):
        total = terms[0].astype(F32)
        for term in terms[1:]:
            total = total + term.astype(F32)
        return total.astype(BF)

    def c_step(slot, i):
        got(RY.at[slot, 0, 0, i], AY + slot * 6 + i)
        G[slot, 0, yp, i + 1] = add(G[slot, 0, yp, i + 1], RY[slot, 0, 0, i])
        copy(G.at[slot, 0, yp, i + 1], RC.at[slot, 0, i], YPd, GC + slot * 6 + i).start()
        got(RY.at[slot, 1, 0, i], AY + slot * 6 + 3 + i)
        G[slot, 1, ym, i + 1] = add(G[slot, 1, ym, i + 1], RY[slot, 1, 0, i])
        copy(G.at[slot, 1, ym, i + 1], RC.at[slot, 1, i], YMd, GC + slot * 6 + 3 + i).start()

    def chain_b(m):
        w, i = m % 2, m // 2 + 1

        @pl.when(root)
        def _():
            copy(G.at[1, w, y, i], ZA.at[m], ZMd, GA + m).start()

        @pl.when(p >= 2)
        def _():
            got(ZB.at[m], GB + m)
            G[1, w, y, i] = add(G[1, w, y, i], ZB[m])

        @pl.when(p != 0)
        def _():
            copy(G.at[1, w, y, i], ZB.at[m], ZPd, GB + m).start()

    def chain_a(m):
        w, i = m % 2, m // 2 + 1
        got(ZA.at[m], GA + m)

        @pl.when(p != 0)
        def _():
            G[0, w, y, i] = add(G[0, w, y, i], ZA[m])
            copy(G.at[0, w, y, i], ZA.at[m], ZMd, GA + m).start()

        @pl.when(root)
        def _():
            got(ZB.at[m], GB + m)
            G[0, w, y, i] = add(G[0, w, y, i], ZA[m], ZB[m])
            copy(G.at[0, w, y, i], FX.at[w], dev(y, (x + i) % 4, z, c), FS + w, FSS + w * 4 + i).start()

    def y_final(slot, i):
        got(RY.at[slot, 1, 1, i], BY + slot * 6 + 3 + i)
        got(RC.at[slot, 0, i], GC + slot * 6 + i)
        G[slot, 0, y, i + 1] = add(G[slot, 0, y, i + 1], RC[slot, 0, i], RY[slot, 1, 1, i])
        got(RY.at[slot, 0, 1, i], BY + slot * 6 + i)
        got(RC.at[slot, 1, i], GC + slot * 6 + 3 + i)
        G[slot, 1, y, i + 1] = add(G[slot, 1, y, i + 1], RC[slot, 1, i], RY[slot, 0, 1, i])

    def qplace(q):
        i = q // 2
        return q % 2, (y + jnp.where(i < 2, 2 - i, i + 1)) % 4

    def own_b(q):
        w, yy = qplace(q)

        @pl.when(root)
        def _():
            copy(G.at[1, w, yy, 0], UA.at[q], ZMd, QA + q).start()

        @pl.when(p >= 2)
        def _():
            got(UB.at[q], QB + q)
            G[1, w, yy, 0] = add(G[1, w, yy, 0], UB[q])

        @pl.when(p != 0)
        def _():
            copy(G.at[1, w, yy, 0], UB.at[q], ZPd, QB + q).start()

    def own_a(q):
        w, yy = qplace(q)
        got(UA.at[q], QA + q)

        @pl.when(p != 0)
        def _():
            G[0, w, yy, 0] = add(G[0, w, yy, 0], UA[q])
            copy(G.at[0, w, yy, 0], UA.at[q], ZMd, QA + q).start()

        @pl.when(root)
        def _():
            got(UB.at[q], QB + q)
            G[0, w, yy, 0] = add(G[0, w, yy, 0], UA[q], UB[q])

            @pl.when(q == 0)
            def _():
                copy(G.at[0, 0, yo, 0], RG.at[0, 0], YPd, RS).start()

            @pl.when(q == 1)
            def _():
                copy(G.at[0, 1, yo, 0], RG.at[1, 0], YMd, RS + 1).start()

            @pl.when(q == 3)
            def _():
                copy(G.at[0, 1, yp, 0], RG.at[0, 1], YPd, RS + 2).start()

            @pl.when(q == 4)
            def _():
                copy(G.at[0, 0, ym, 0], RG.at[1, 1], YMd, RS + 3).start()

    def igrad(n):
        rows = pl.ds(pl.multiple_of(n * 256, 256), 256)
        nt = (((1,), (1,)), ((), ()))
        part = lax.dot_general(DP[0], W[0, 0, rows, :], nt, preferred_element_type=F32)
        part = part + lax.dot_general(DP[1], W[1, 0, rows, :], nt, preferred_element_type=F32)
        part = part.astype(BF).reshape(4, 2, 128, 256)
        cols = pl.ds(pl.multiple_of((n % 4) * 256, 256), 256)
        for cc in range(2):
            S[cc, n // 4, :, :, cols] = part[:, cc]

    act(far, 2)
    grads(far, True)

    b_send(far, 0)
    act(near, 2)
    c_step(far, 0)
    b_send(far, 1)
    grads(near, False, 0, 2)
    c_step(far, 1)
    b_send(far, 2)
    grads(near, False, 2, 2)
    c_step(far, 2)
    both(3, lambda i: a_send(near, i))
    b_send(near, 0)

    def x_first(half):
        got(RP.at[half], XC + half)
        both(4, lambda r: xadd(half, r))

    def xadd(half, r):
        S[c, half, r] = add(S[c, half, r], RP[half, r])

    def x_send():
        copy(S.at[c, 0, xo], XR.at[0, 0], XP, XY).start()
        copy(S.at[c, 1, xo], XR.at[1, 0], XM, XY + 1).start()
        copy(S.at[c, 1, xp], XR.at[0, 1], XP, XY + 2).start()
        copy(S.at[c, 0, xm], XR.at[1, 1], XM, XY + 3).start()

    def x_second():
        got(XR.at[0, 0], XY)
        S[c, 0, xp] = add(S[c, 0, xp], XR[0, 0])
        copy(S.at[c, 0, xp], XR.at[0, 2], XP, XY + 4).start()
        got(XR.at[1, 0], XY + 1)
        S[c, 1, xm] = add(S[c, 1, xm], XR[1, 0])
        copy(S.at[c, 1, xm], XR.at[1, 2], XM, XY + 5).start()

    def root_second():
        got(RG.at[0, 0], RS)
        G[0, 0, yp, 0] = add(G[0, 0, yp, 0], RG[0, 0])
        copy(G.at[0, 0, yp, 0], RG.at[0, 2], YPd, RS + 4).start()
        got(RG.at[1, 0], RS + 1)
        G[0, 1, ym, 0] = add(G[0, 1, ym, 0], RG[1, 0])
        copy(G.at[0, 1, ym, 0], RG.at[1, 2], YMd, RS + 5).start()

    def by_p(*values):
        return jnp.where(p == 0, values[0], jnp.where(p == 1, values[1], jnp.where(p == 2, values[2], values[3])))

    never = 99
    at_own_b = by_p(never, never, 0, 3)
    at_own_a = by_p(9, 6, 3, 0)
    at_chain_a = by_p(18, 15, 12, 9)
    at_chain_b = by_p(never, never, never, 15)

    def rstep(t):
        def span(start, count, body):
            @pl.when((t >= start) & (t < start + count))
            def _():
                body(t - start)

        span(at_own_b, 8, own_b)
        span(at_own_a, 8, own_a)
        span(at_chain_b, 6, chain_b)

        @pl.when(root & (t == 18))
        def _():
            root_second()

        span(at_chain_a, 6, chain_a)

        @pl.when(t < 4)
        def _():
            igrad(t * 2)
            igrad(t * 2 + 1)

        @pl.when((t == 1) | (t == 3))
        def _():
            half = t // 2
            copy(S.at[1 - c, half], RP.at[half], PA, XC + half).start()

        @pl.when((t == 4) | (t == 5) | (t == 7))
        def _():
            i = (t - 3) // 2
            y_final(far, i)

            @pl.when(p < 2)
            def _():
                chain_b(i * 2)
                chain_b(i * 2 + 1)

        @pl.when((t == 5) | (t == 6))
        def _():
            x_first(t - 5)

        @pl.when(t == 6)
        def _():
            x_send()

        @pl.when((t >= 8) & (t < 11))
        def _():
            i = t - 8
            c_step(near, i)

            @pl.when(i < 2)
            def _():
                b_send(near, i + 1)

        @pl.when(t == 13)
        def _():
            x_second()

        @pl.when((t == 12) | (t == 14) | (t == 16))
        def _():
            i = (t - 12) // 2
            y_final(near, i)

            @pl.when(p == 2)
            def _():
                chain_b(i * 2)
                chain_b(i * 2 + 1)

    both(24, rstep)

    got(XR.at[0, 1], XY + 2)
    got(XR.at[1, 1], XY + 3)
    got(XR.at[0, 2], XY + 4)
    got(XR.at[1, 2], XY + 5)
    for half, (d0, k0), (d1, k1) in ((0, (0, 2), (1, 1)), (1, (0, 1), (1, 2))):
        ig_out[:, half * 1024 : (half + 1) * 1024] = add(S[c, half, x], XR[d0, k0], XR[d1, k1])

    @pl.when(root)
    def _():
        for k in range(1, 5):
            got(RG.at[(k + 1) % 2, (k + 1) // 2], RS + k + 1)
        FX[0] = add(G[0, 0, y, 0], RG[0, 2], RG[1, 1])
        FX[1] = add(G[0, 1, y, 0], RG[0, 1], RG[1, 2])

    @pl.when(p != 0)
    def _():
        for w in range(2):
            got(FX.at[w], FS + w)

    ug_out[...] = FX[0].astype(F32).T * factor
    dg_out[...] = FX[1].astype(F32) * factor

    unit = FX.at[0]

    @pl.when(p != 0)
    def _():
        for w in range(2):
            sent(unit, SX + w * 4 + x)

    def chain_sends(m):
        sent(unit, ZP + m)

        @pl.when(p != 1)
        def _():
            sent(unit, ZM + m)

    both(14, chain_sends)

    def sends(k):
        w, j = k // 4, k % 4
        for slot in range(2):

            @pl.when((j != x) | (root & (slot == 0)))
            def _(slot=slot):
                for base in (YP, YM, YF):
                    sent(unit, base + slot * 8 + k)

        sent(UA.at[k], QA + k)

        @pl.when(p != 0)
        def _():
            sent(UB.at[k], QB + k)

        @pl.when(root & (j != 0))
        def _():
            sent(unit, FSS + k)

        sent(xblock(w, x, crow), TC + k)

    both(8, sends)

    def more_sends(m):
        sent(unit, GC + m)
        sent(unit, GC + 6 + m)
        for base in (AY, BY):
            sent(unit, base + m)
            sent(unit, base + 6 + m)
        sent(unit, GA + m)

        @pl.when(p != 0)
        def _():
            sent(unit, GB + m)

        @pl.when(root)
        def _():
            sent(unit, RS + m)

        sent(xblock(0, x, crow), TP + m)
        sent(XR.at[0, 0], XY + m)

    both(6, more_sends)
    for i in range(2):
        sent(RP.at[0], XC + i)


def solution(mesh):
    def shards(tokens, up_weight, down_weight, cotangent):
        count_all = tokens.shape[0] * lax.axis_size("fs") * lax.axis_size("tp")
        factor = 1.0 / float(count_all) ** 0.5
        vmem = pl.BlockSpec(memory_space=pltpu.VMEM)
        hbm = pl.BlockSpec(memory_space=pl.ANY)

        def body(*refs):
            kernel(factor, *refs)

        return pl.pallas_call(
            body,
            out_shape=(
                jax.ShapeDtypeStruct((128, 2048), BF),
                jax.ShapeDtypeStruct((128, 256), F32),
                jax.ShapeDtypeStruct((256, 128), F32),
            ),
            in_specs=[hbm, vmem, vmem, hbm],
            out_specs=(vmem, vmem, vmem),
            scratch_shapes=[
                pltpu.VMEM((2, 4, 256, 2048), BF),
                pltpu.VMEM((2, 128, 256), BF),
                pltpu.VMEM((2, 2, 2048, 256), BF),
                pltpu.VMEM((2, 1024, 256), BF),
                pltpu.VMEM((2, 2, 256, 1024), BF),
                pltpu.VMEM((2, 2, 4, 4, 256, 128), BF),
                pltpu.VMEM((2, 2, 2, 3, 256, 128), BF),
                pltpu.VMEM((2, 2, 3, 256, 128), BF),
                pltpu.VMEM((6, 256, 128), BF),
                pltpu.VMEM((6, 256, 128), BF),
                pltpu.VMEM((8, 256, 128), BF),
                pltpu.VMEM((8, 256, 128), BF),
                pltpu.VMEM((2, 3, 256, 128), BF),
                pltpu.VMEM((2, 256, 128), BF),
                pltpu.VMEM((2, 2, 4, 128, 1024), BF),
                pltpu.VMEM((2, 4, 128, 1024), BF),
                pltpu.VMEM((2, 3, 128, 1024), BF),
                pltpu.SemaphoreType.DMA((N_SEM,)),
                pltpu.SemaphoreType.DMA((N_SEM,)),
                pltpu.SemaphoreType.DMA((2,)),
            ],
            compiler_params=pltpu.CompilerParams(
                collective_id=0, has_side_effects=True, vmem_limit_bytes=54250 * 1024
            ),
            name="ffn_backward",
        )(tokens, up_weight, down_weight, cotangent)

    placed = (P(("fs", "tp"), None), P("fs", "tp"), P("tp", "fs"), P(("fs", "tp"), None))
    return jax.shard_map(
        shards,
        mesh=mesh,
        in_specs=placed,
        out_specs=(P(("fs", "tp"), None), P("fs", "tp"), P("tp", "fs")),
        check_vma=False,
    )
```

```python
import jax
import jax.numpy as jnp
from jax import lax
from jax.experimental import pallas as pl
from jax.experimental.pallas import tpu as pltpu
from jax.sharding import PartitionSpec as P

BF = jnp.bfloat16
F32 = jnp.float32
MESH = pl.DeviceIdType.MESH

SX, ZP, ZM, YP, YM, YF = 0, 8, 22, 36, 52, 68
TP, TM, TF, TC = 84, 86, 88, 90
AY, BY, GC, GA, GB, QA, QB, RS = 98, 110, 122, 134, 140, 146, 154, 162
FS, FSS, XC, XY = 168, 170, 178, 180
N_SEM = 186


def both(n, body):
    def step(i, carry):
        body(i)
        return carry

    lax.fori_loop(0, n, step, 0)


def kernel(
    factor, tok_in, up_in, dn_in, cot_in, ig_out, ug_out, dg_out,
    X, WS, W, DP, TT, G, RY, RC, ZA, ZB, UA, UB, RG, FX, S, RP, XR, ssem, rsem, lsem,
):
    fs, tp = lax.axis_index("fs"), lax.axis_index("tp")
    y, x = fs // 4, fs % 4
    z, c = tp // 2, tp % 2
    p = lax.rem(z - x + 8, 4)
    xp, xm, xo = (x + 1) % 4, (x + 3) % 4, (x + 2) % 4
    yp, ym, yo = (y + 1) % 4, (y + 3) % 4, (y + 2) % 4
    zp, zm = (z + 1) % 8, (z + 7) % 8

    def dev(yy, xx, zz, cc):
        return (yy * 4 + xx, zz * 2 + cc)

    XP, XM, XO = dev(y, xp, z, c), dev(y, xm, z, c), dev(y, xo, z, c)
    YPd, YMd = dev(yp, x, z, c), dev(ym, x, z, c)
    ZPd, ZMd = dev(y, x, zp, c), dev(y, x, zm, c)
    PA = dev(y, x, z, 1 - c)

    def copy(src, dst, to, sid, sent_id=None):
        sent_id = sid if sent_id is None else sent_id
        return pltpu.make_async_remote_copy(
            src_ref=src, dst_ref=dst, send_sem=ssem.at[sent_id], recv_sem=rsem.at[sid],
            device_id=to, device_id_type=MESH,
        )

    def got(ref, sid):
        copy(ref, ref, PA, sid).wait_recv()

    def sent(ref, sid):
        copy(ref, ref, PA, sid).wait_send()

    crow = pl.ds(pl.multiple_of(c * 128, 128), 128)
    own = [pltpu.make_async_copy(a, X.at[w, x, crow, :], lsem.at[w]) for w, a in enumerate((tok_in, cot_in))]
    for o in own:
        o.start()
    WS[0] = up_in[...]
    WS[1] = dn_in[...].astype(F32).T.astype(BF)

    barrier = pltpu.get_barrier_semaphore()
    for to in (XP, XM, XO, YPd, YMd, ZPd, ZMd, PA):
        pl.semaphore_signal(barrier, inc=1, device_id=to, device_id_type=MESH)
    pl.semaphore_wait(barrier, 8)

    def wrow(yy, j):
        return pl.ds(pl.multiple_of(yy * 512 + j * 128, 128), 128)

    def wpiece(slot, w, yy, j):
        return W.at[slot, w, wrow(yy, j), :]

    @pl.when(p != 0)
    def _():
        for w in range(2):
            copy(WS.at[w], wpiece(0, w, y, x), dev(y, (x + p) % 4, z, c), SX + w * 4 + x).start()

    for o in own:
        o.wait()

    def xblock(w, xx, cc_row):
        return X.at[w, xx, cc_row, :]

    for w, to, base in ((0, XP, TP), (1, XM, TM), (1, XP, TP), (0, XM, TM)):
        copy(xblock(w, x, crow), xblock(w, x, crow), to, base + w).start()
    for w in range(2):
        copy(xblock(w, x, crow), xblock(w, x, crow), PA, TC + w * 4).start()

    def ysend(slot, w, j):
        piece = wpiece(slot, w, y, j)
        copy(piece, piece, YPd, YP + slot * 8 + w * 4 + j).start()
        copy(piece, piece, YMd, YM + slot * 8 + w * 4 + j).start()

    @pl.when(p == 0)
    def _():
        for w in range(2):
            W[0, w, wrow(y, x), :] = WS[w]
            ysend(0, w, x)

    def root_forward():
        got(wpiece(0, 0, ym, x), YP + x)
        copy(wpiece(0, 0, ym, x), wpiece(0, 0, ym, x), YPd, YF + x).start()
        got(wpiece(0, 1, yp, x), YM + 4 + x)
        copy(wpiece(0, 1, yp, x), wpiece(0, 1, yp, x), YMd, YF + 4 + x).start()

    def root_rest():
        got(wpiece(0, 0, yp, x), YM + x)
        got(wpiece(0, 1, ym, x), YP + 4 + x)
        for w in range(2):
            got(wpiece(0, w, yo, x), YF + w * 4 + x)

    def place(m):
        w, i = m % 2, m // 2
        return w, jnp.where(i < 4, y, (y + i + 1) % 4), jnp.where(i < 4, (x + i) % 4, x)

    def step_a(m):
        w, yy, j = place(m)
        piece = wpiece(0, w, yy, j)

        @pl.when((p == 0) & (m >= 2) & (m < 8))
        def _():
            got(piece, SX + w * 4 + j)

        @pl.when(p != 0)
        def _():
            got(piece, ZP + m)

        copy(piece, wpiece(jnp.where(p == 3, 1, 0), w, yy, j), ZPd, ZP + m).start()

        @pl.when(p == 0)
        def _():
            copy(piece, wpiece(1, w, yy, j), ZMd, ZM + m).start()

        @pl.when((m >= 2) & (m < 8))
        def _():
            ysend(0, w, j)

    def step_b(m):
        w, yy, j = place(m)
        piece = wpiece(1, w, yy, j)

        @pl.when(p == 0)
        def _():
            got(piece, ZP + m)

        @pl.when(p != 0)
        def _():
            got(piece, ZM + m)

        @pl.when(p >= 2)
        def _():
            copy(piece, piece, ZMd, ZM + m).start()

        @pl.when((m >= 2) & (m < 8))
        def _():
            ysend(1, w, j)

    def yforward(slot, m):
        w, j = m % 2, (x + m // 2 + 1) % 4

        @pl.when(w == 0)
        def _():
            piece = wpiece(slot, 0, ym, j)
            got(piece, YP + slot * 8 + j)
            copy(piece, piece, YPd, YF + slot * 8 + j).start()

        @pl.when(w == 1)
        def _():
            piece = wpiece(slot, 1, yp, j)
            got(piece, YM + slot * 8 + 4 + j)
            copy(piece, piece, YMd, YF + slot * 8 + 4 + j).start()

    def pass_on(w, r):
        xx = (x + r) % 4
        copy(xblock(w, xx, crow), xblock(w, xx, crow), PA, TC + w * 4 + r).start()

    near = jnp.where(p < 2, 0, 1)
    far = 1 - near
    root = p == 0
    lag_a = jnp.where(p == 3, 5, 0)
    lag_b = jnp.where(root, 20, jnp.where(p == 1, 5, 0))
    lag_far = jnp.where(root, 24, jnp.where(p == 2, 10, 15))

    def yfinish(slot):
        def piece(i):
            j = (x + i + 1) % 4
            got(wpiece(slot, 0, yp, j), YM + slot * 8 + j)
            got(wpiece(slot, 1, ym, j), YP + slot * 8 + 4 + j)
            for w in range(2):
                got(wpiece(slot, w, yo, j), YF + slot * 8 + w * 4 + j)

        both(3, piece)

    orow = pl.ds(pl.multiple_of((1 - c) * 128, 128), 128)

    def partner(r):
        for w in range(2):
            got(xblock(w, (x + r) % 4, orow), TC + w * 4 + r)

    def act(slot, r):
        xx = (x + r) % 4
        pre = jnp.dot(X[0, xx], W[slot, 0], preferred_element_type=F32)
        dh = jnp.dot(X[1, xx], W[slot, 1], preferred_element_type=F32)
        active = jnp.maximum(pre, 0.0)
        hidden = active * active
        dpre = 2.0 * active * dh
        DP[slot, pl.ds(pl.multiple_of(xx * 256, 256), 256), :] = dpre.astype(BF)
        cols = pl.ds(pl.multiple_of(xx * 256, 256), 256)
        TT[slot, 0, :, cols] = dpre.T.astype(BF)
        TT[slot, 1, :, cols] = hidden.T.astype(BF)

    def act_three(slot):
        both(3, lambda i: act(slot, jnp.where(i == 2, 3, i)))

    def near_part():
        yfinish(near)
        partner(0)
        partner(1)
        partner(3)
        act_three(near)

    def zstep(t):
        @pl.when(root & (t == 2))
        def _():
            root_forward()

        @pl.when(root & (t == 6))
        def _():
            root_rest()

        @pl.when((t >= lag_a) & (t < lag_a + 14))
        def _():
            step_a(t - lag_a)

        @pl.when((t >= lag_b) & (t < lag_b + 14))
        def _():
            step_b(t - lag_b)

        @pl.when(t == jnp.where(root, 14, 8))
        def _():
            got(xblock(0, xm, crow), TP)
            copy(xblock(0, xm, crow), xblock(0, xm, crow), XP, TF).start()
            got(xblock(1, xp, crow), TM + 1)
            copy(xblock(1, xp, crow), xblock(1, xp, crow), XM, TF + 1).start()
            pass_on(0, 3)
            pass_on(1, 1)

        @pl.when(root & (t >= 14) & (t < 20))
        def _():
            yforward(near, t - 14)

        @pl.when((p != 0) & (t >= 6) & (t < 18) & (t % 2 == 0))
        def _():
            yforward(near, (t - 6) // 2)

        @pl.when((t >= lag_far) & (t < lag_far + 6))
        def _():
            yforward(far, t - lag_far)

        @pl.when(t == jnp.where(root, 26, 15))
        def _():
            got(xblock(1, xm, crow), TP + 1)
            pass_on(1, 3)
            got(xblock(0, xp, crow), TM)
            pass_on(0, 1)

        @pl.when(root & (t == 30))
        def _():
            near_part()

    both(34, zstep)

    pl.when(p != 0)(near_part)
    got(xblock(0, xo, crow), TF)
    pass_on(0, 2)
    got(xblock(1, xo, crow), TF + 1)
    pass_on(1, 2)
    yfinish(far)
    act_three(far)
    partner(2)

    def grads(slot, send, first=0, count=4):
        def block(i):
            yy = (y + jnp.where(i < 2, 2 - i, i + 1)) % 4
            cols = pl.ds(pl.multiple_of(yy * 512, 512), 512)
            for w in range(2):
                rows = X[w, :, :, cols].reshape(1024, 512)
                part = jnp.dot(TT[slot, w], rows, preferred_element_type=F32).astype(BF)
                for j in range(4):
                    G[slot, w, yy, (j - x + 4) % 4] = part[:, j * 128 : (j + 1) * 128]
                if send:

                    @pl.when(p < 2)
                    def _(w=w):
                        own_b(2 * i + w)

                    @pl.when(i == 0)
                    def _(w=w):
                        both(3, lambda n: a_send(slot, n, w))

        both(count, lambda i: block(first + i))

    def a_send(slot, i, w):
        to = (YPd, YMd)[w]
        copy(G.at[slot, w, yo, i + 1], RY.at[slot, w, 0, i], to, AY + slot * 6 + w * 3 + i).start()

    def b_send(slot, i):
        copy(G.at[slot, 1, yp, i + 1], RY.at[slot, 0, 1, i], YPd, BY + slot * 6 + i).start()
        copy(G.at[slot, 0, ym, i + 1], RY.at[slot, 1, 1, i], YMd, BY + slot * 6 + 3 + i).start()

    def add(*terms):
        total = terms[0].astype(F32)
        for term in terms[1:]:
            total = total + term.astype(F32)
        return total.astype(BF)

    def c_step(slot, i):
        got(RY.at[slot, 0, 0, i], AY + slot * 6 + i)
        G[slot, 0, yp, i + 1] = add(G[slot, 0, yp, i + 1], RY[slot, 0, 0, i])
        copy(G.at[slot, 0, yp, i + 1], RC.at[slot, 0, i], YPd, GC + slot * 6 + i).start()
        got(RY.at[slot, 1, 0, i], AY + slot * 6 + 3 + i)
        G[slot, 1, ym, i + 1] = add(G[slot, 1, ym, i + 1], RY[slot, 1, 0, i])
        copy(G.at[slot, 1, ym, i + 1], RC.at[slot, 1, i], YMd, GC + slot * 6 + 3 + i).start()

    def chain_b(m):
        w, i = m % 2, m // 2 + 1

        @pl.when(root)
        def _():
            copy(G.at[1, w, y, i], ZA.at[m], ZMd, GA + m).start()

        @pl.when(p >= 2)
        def _():
            got(ZB.at[m], GB + m)
            G[1, w, y, i] = add(G[1, w, y, i], ZB[m])

        @pl.when(p != 0)
        def _():
            copy(G.at[1, w, y, i], ZB.at[m], ZPd, GB + m).start()

    def chain_a(m):
        w, i = m % 2, m // 2 + 1
        got(ZA.at[m], GA + m)

        @pl.when(p != 0)
        def _():
            G[0, w, y, i] = add(G[0, w, y, i], ZA[m])
            copy(G.at[0, w, y, i], ZA.at[m], ZMd, GA + m).start()

        @pl.when(root)
        def _():
            got(ZB.at[m], GB + m)
            G[0, w, y, i] = add(G[0, w, y, i], ZA[m], ZB[m])
            copy(G.at[0, w, y, i], FX.at[w], dev(y, (x + i) % 4, z, c), FS + w, FSS + w * 4 + i).start()

    def y_final(slot, i):
        got(RY.at[slot, 1, 1, i], BY + slot * 6 + 3 + i)
        got(RC.at[slot, 0, i], GC + slot * 6 + i)
        G[slot, 0, y, i + 1] = add(G[slot, 0, y, i + 1], RC[slot, 0, i], RY[slot, 1, 1, i])
        got(RY.at[slot, 0, 1, i], BY + slot * 6 + i)
        got(RC.at[slot, 1, i], GC + slot * 6 + 3 + i)
        G[slot, 1, y, i + 1] = add(G[slot, 1, y, i + 1], RC[slot, 1, i], RY[slot, 0, 1, i])

    def qplace(q):
        i = q // 2
        return q % 2, (y + jnp.where(i < 2, 2 - i, i + 1)) % 4

    def own_b(q):
        w, yy = qplace(q)

        @pl.when(root)
        def _():
            copy(G.at[1, w, yy, 0], UA.at[q], ZMd, QA + q).start()

        @pl.when(p >= 2)
        def _():
            got(UB.at[q], QB + q)
            G[1, w, yy, 0] = add(G[1, w, yy, 0], UB[q])

        @pl.when(p != 0)
        def _():
            copy(G.at[1, w, yy, 0], UB.at[q], ZPd, QB + q).start()

    def own_a(q):
        w, yy = qplace(q)
        got(UA.at[q], QA + q)

        @pl.when(p != 0)
        def _():
            G[0, w, yy, 0] = add(G[0, w, yy, 0], UA[q])
            copy(G.at[0, w, yy, 0], UA.at[q], ZMd, QA + q).start()

        @pl.when(root)
        def _():
            got(UB.at[q], QB + q)
            G[0, w, yy, 0] = add(G[0, w, yy, 0], UA[q], UB[q])

            @pl.when(q == 0)
            def _():
                copy(G.at[0, 0, yo, 0], RG.at[0, 0], YPd, RS).start()

            @pl.when(q == 1)
            def _():
                copy(G.at[0, 1, yo, 0], RG.at[1, 0], YMd, RS + 1).start()

            @pl.when(q == 3)
            def _():
                copy(G.at[0, 1, yp, 0], RG.at[0, 1], YPd, RS + 2).start()

            @pl.when(q == 4)
            def _():
                copy(G.at[0, 0, ym, 0], RG.at[1, 1], YMd, RS + 3).start()

    def igrad(n):
        rows = pl.ds(pl.multiple_of(n * 256, 256), 256)
        nt = (((1,), (1,)), ((), ()))
        part = lax.dot_general(DP[0], W[0, 0, rows, :], nt, preferred_element_type=F32)
        part = part + lax.dot_general(DP[1], W[1, 0, rows, :], nt, preferred_element_type=F32)
        part = part.astype(BF).reshape(4, 2, 128, 256)
        cols = pl.ds(pl.multiple_of((n % 4) * 256, 256), 256)
        for cc in range(2):
            S[cc, n // 4, :, :, cols] = part[:, cc]

    act(far, 2)
    grads(far, True)

    b_send(far, 0)
    act(near, 2)
    c_step(far, 0)
    b_send(far, 1)
    grads(near, False, 0, 2)
    c_step(far, 1)
    b_send(far, 2)
    grads(near, False, 2, 2)
    c_step(far, 2)
    for w in range(2):
        both(3, lambda i, w=w: a_send(near, i, w))
    b_send(near, 0)

    def x_first(half):
        got(RP.at[half], XC + half)
        both(4, lambda r: xadd(half, r))

    def xadd(half, r):
        S[c, half, r] = add(S[c, half, r], RP[half, r])

    def x_send():
        copy(S.at[c, 0, xo], XR.at[0, 0], XP, XY).start()
        copy(S.at[c, 1, xo], XR.at[1, 0], XM, XY + 1).start()
        copy(S.at[c, 1, xp], XR.at[0, 1], XP, XY + 2).start()
        copy(S.at[c, 0, xm], XR.at[1, 1], XM, XY + 3).start()

    def x_second():
        got(XR.at[0, 0], XY)
        S[c, 0, xp] = add(S[c, 0, xp], XR[0, 0])
        copy(S.at[c, 0, xp], XR.at[0, 2], XP, XY + 4).start()
        got(XR.at[1, 0], XY + 1)
        S[c, 1, xm] = add(S[c, 1, xm], XR[1, 0])
        copy(S.at[c, 1, xm], XR.at[1, 2], XM, XY + 5).start()

    def root_second():
        got(RG.at[0, 0], RS)
        G[0, 0, yp, 0] = add(G[0, 0, yp, 0], RG[0, 0])
        copy(G.at[0, 0, yp, 0], RG.at[0, 2], YPd, RS + 4).start()
        got(RG.at[1, 0], RS + 1)
        G[0, 1, ym, 0] = add(G[0, 1, ym, 0], RG[1, 0])
        copy(G.at[0, 1, ym, 0], RG.at[1, 2], YMd, RS + 5).start()

    def by_p(*values):
        return jnp.where(p == 0, values[0], jnp.where(p == 1, values[1], jnp.where(p == 2, values[2], values[3])))

    never = 99
    at_own_b = by_p(never, never, 0, 3)
    at_own_a = by_p(9, 6, 3, 0)
    at_chain_a = by_p(18, 15, 12, 9)
    at_chain_b = by_p(never, never, never, 15)

    def rstep(t):
        def span(start, count, body):
            @pl.when((t >= start) & (t < start + count))
            def _():
                body(t - start)

        span(at_own_b, 8, own_b)
        span(at_own_a, 8, own_a)
        span(at_chain_b, 6, chain_b)

        @pl.when(root & (t == 18))
        def _():
            root_second()

        span(at_chain_a, 6, chain_a)

        @pl.when(t < 4)
        def _():
            igrad(t * 2)
            igrad(t * 2 + 1)

        @pl.when((t == 1) | (t == 3))
        def _():
            half = t // 2
            copy(S.at[1 - c, half], RP.at[half], PA, XC + half).start()

        @pl.when((t == 4) | (t == 5) | (t == 7))
        def _():
            i = (t - 3) // 2
            y_final(far, i)

            @pl.when(p < 2)
            def _():
                chain_b(i * 2)
                chain_b(i * 2 + 1)

        @pl.when((t == 5) | (t == 6))
        def _():
            x_first(t - 5)

        @pl.when(t == 6)
        def _():
            x_send()

        @pl.when((t >= 8) & (t < 11))
        def _():
            i = t - 8
            c_step(near, i)

            @pl.when(i < 2)
            def _():
                b_send(near, i + 1)

        @pl.when(t == 13)
        def _():
            x_second()

        @pl.when((t == 12) | (t == 14) | (t == 16))
        def _():
            i = (t - 12) // 2
            y_final(near, i)

            @pl.when(p == 2)
            def _():
                chain_b(i * 2)
                chain_b(i * 2 + 1)

    both(24, rstep)

    got(XR.at[0, 1], XY + 2)
    got(XR.at[1, 1], XY + 3)
    got(XR.at[0, 2], XY + 4)
    got(XR.at[1, 2], XY + 5)
    for half, (d0, k0), (d1, k1) in ((0, (0, 2), (1, 1)), (1, (0, 1), (1, 2))):
        ig_out[:, half * 1024 : (half + 1) * 1024] = add(S[c, half, x], XR[d0, k0], XR[d1, k1])

    @pl.when(root)
    def _():
        for k in range(1, 5):
            got(RG.at[(k + 1) % 2, (k + 1) // 2], RS + k + 1)
        FX[0] = add(G[0, 0, y, 0], RG[0, 2], RG[1, 1])
        FX[1] = add(G[0, 1, y, 0], RG[0, 1], RG[1, 2])

    @pl.when(p != 0)
    def _():
        for w in range(2):
            got(FX.at[w], FS + w)

    ug_out[...] = FX[0].astype(F32).T * factor
    dg_out[...] = FX[1].astype(F32) * factor

    unit = FX.at[0]

    @pl.when(p != 0)
    def _():
        for w in range(2):
            sent(unit, SX + w * 4 + x)

    def chain_sends(m):
        sent(unit, ZP + m)

        @pl.when(p != 1)
        def _():
            sent(unit, ZM + m)

    both(14, chain_sends)

    def sends(k):
        w, j = k // 4, k % 4
        for slot in range(2):

            @pl.when((j != x) | (root & (slot == 0)))
            def _(slot=slot):
                for base in (YP, YM, YF):
                    sent(unit, base + slot * 8 + k)

        sent(UA.at[k], QA + k)

        @pl.when(p != 0)
        def _():
            sent(UB.at[k], QB + k)

        @pl.when(root & (j != 0))
        def _():
            sent(unit, FSS + k)

        sent(xblock(w, x, crow), TC + k)

    both(8, sends)

    def more_sends(m):
        sent(unit, GC + m)
        sent(unit, GC + 6 + m)
        for base in (AY, BY):
            sent(unit, base + m)
            sent(unit, base + 6 + m)
        sent(unit, GA + m)

        @pl.when(p != 0)
        def _():
            sent(unit, GB + m)

        @pl.when(root)
        def _():
            sent(unit, RS + m)

        sent(xblock(0, x, crow), TP + m)
        sent(XR.at[0, 0], XY + m)

    both(6, more_sends)
    for i in range(2):
        sent(RP.at[0], XC + i)


def solution(mesh):
    def shards(tokens, up_weight, down_weight, cotangent):
        count_all = tokens.shape[0] * lax.axis_size("fs") * lax.axis_size("tp")
        factor = 1.0 / float(count_all) ** 0.5
        vmem = pl.BlockSpec(memory_space=pltpu.VMEM)
        hbm = pl.BlockSpec(memory_space=pl.ANY)

        def body(*refs):
            kernel(factor, *refs)

        return pl.pallas_call(
            body,
            out_shape=(
                jax.ShapeDtypeStruct((128, 2048), BF),
                jax.ShapeDtypeStruct((128, 256), F32),
                jax.ShapeDtypeStruct((256, 128), F32),
            ),
            in_specs=[hbm, vmem, vmem, hbm],
            out_specs=(vmem, vmem, vmem),
            scratch_shapes=[
                pltpu.VMEM((2, 4, 256, 2048), BF),
                pltpu.VMEM((2, 128, 256), BF),
                pltpu.VMEM((2, 2, 2048, 256), BF),
                pltpu.VMEM((2, 1024, 256), BF),
                pltpu.VMEM((2, 2, 256, 1024), BF),
                pltpu.VMEM((2, 2, 4, 4, 256, 128), BF),
                pltpu.VMEM((2, 2, 2, 3, 256, 128), BF),
                pltpu.VMEM((2, 2, 3, 256, 128), BF),
                pltpu.VMEM((6, 256, 128), BF),
                pltpu.VMEM((6, 256, 128), BF),
                pltpu.VMEM((8, 256, 128), BF),
                pltpu.VMEM((8, 256, 128), BF),
                pltpu.VMEM((2, 3, 256, 128), BF),
                pltpu.VMEM((2, 256, 128), BF),
                pltpu.VMEM((2, 2, 4, 128, 1024), BF),
                pltpu.VMEM((2, 4, 128, 1024), BF),
                pltpu.VMEM((2, 3, 128, 1024), BF),
                pltpu.SemaphoreType.DMA((N_SEM,)),
                pltpu.SemaphoreType.DMA((N_SEM,)),
                pltpu.SemaphoreType.DMA((2,)),
            ],
            compiler_params=pltpu.CompilerParams(
                collective_id=0, has_side_effects=True, vmem_limit_bytes=54250 * 1024
            ),
            name="ffn_backward",
        )(tokens, up_weight, down_weight, cotangent)

    placed = (P(("fs", "tp"), None), P("fs", "tp"), P("tp", "fs"), P(("fs", "tp"), None))
    return jax.shard_map(
        shards,
        mesh=mesh,
        in_specs=placed,
        out_specs=(P(("fs", "tp"), None), P("fs", "tp"), P("tp", "fs")),
        check_vma=False,
    )
```
